512 devices in a mesh: ep: 16 (over y, x), tp: 32 (over z, core).
Axes of the slice: x: 4, y: 4, z: 16, core: 2. Of those that a mesh axis runs over, the one named last changes fastest.
Arguments:
- tokens: bfloat16 [3072, 4096], P('ep', 'tp'), may hold values from -6 to 6
- cotangent: bfloat16 [3072, 4096], P('ep', 'tp'), may hold values from -4 to 4
- routes: int32 [3072, 2], P('ep'), may hold values from 0 to 31, all different within a row; in each aligned block of 192 rows (0 to 191, 192 to 383, ...) at most 18 rows name the same one
- gate_weights: bfloat16 [3072, 2], P('ep'), may hold values from 0.099609375 to 2.5
- expert_gate: bfloat16 [32, 4096, 1024], P('ep', 'tp'), may hold values from -0.09375 to 0.09375
- expert_up: bfloat16 [32, 4096, 1024], P('ep', 'tp'), may hold values from -0.09375 to 0.09375
- expert_down: bfloat16 [32, 4096, 1024], P('ep', 'tp'), may hold values from -0.1875 to 0.1875
- shared_gate: bfloat16 [4096, 1024], P('tp'), may hold values from -0.09375 to 0.09375
- shared_up: bfloat16 [4096, 1024], P('tp'), may hold values from -0.09375 to 0.09375
- shared_down: bfloat16 [4096, 1024], P('tp'), may hold values from -0.1875 to 0.1875
Outputs:
- token_grad: bfloat16 [3072, 4096], P('ep', 'tp')
- gate_grad: bfloat16 [3072, 2], P('ep')
- expert_grads: bfloat16 [3, 32, 4096, 1024], P(None, 'ep', 'tp')
- shared_grads: float32 [3, 4096, 1024], P(None, 'tp', 'ep')
- expert_norms: float32 [3, 32, 1024], P(None, 'ep')
- shared_norms: float32 [3, 1024], P(None, 'ep')
The draws below stay inside these ranges and needn't reach their ends.
Inputs may be any that keep to these rules, and one draw needn't show every extreme that they name: `routes`: each row names 2 different experts. In each aligned block of 192 rows no expert is named by more than 18 rows, a bound that some block reaches.
All inputs are finite; a program needn't handle non-finite values.
Results may differ from the reference program's by a relative error of at most 0.0069.
Values may be sent and summed in bfloat16 or wider, within the bound.
No kernel may reach another device: no remote copies, remote signals or barrier semaphores. Data moves between devices by JAX's collectives and lax.ppermute only.
A program may use at most 64 MiB of HBM per device.

```python
import math
import jax
import jax.numpy as jnp
import numpy as np
from jax import lax

D = 4096
F = 1024
TOPK = 2
TOK_GRP = 192
EXPERTS = 32
TOKENS = 3072
CAP = 18
N_EP = 16
N_TP = 32


def block_levels(rng, extent, cuts, low, high):
    def one(dim, blocks):
        steps = jax.random.uniform(jax.random.fold_in(jax.random.fold_in(rng, 6), dim), (blocks,), jnp.float32, low / len(cuts), high / len(cuts))
        return jnp.repeat(jnp.exp(steps), extent[dim] // blocks).reshape((-1,) + (1,) * (len(extent) - dim - 1))

    gain = one(*cuts[0])
    for cut in cuts[1:]:
        gain = gain * one(*cut)
    return gain


def shared_out(stream_key, own, number, rows, amount, top, limit, lean):
    sequence = jax.random.permutation(stream_key, amount)
    crowded, ordinary = portions_of(amount, rows * top, limit, lean, True), portions_of(amount, rows * top, limit, lean, False)
    places = jnp.arange(amount)

    def named(sizes, turn):
        used = int((sizes > 0).sum())
        fixed = max(1, used // 4)
        passed = fixed + (places - fixed + turn * (used - fixed)) % max(1, amount - fixed)
        return jnp.zeros((amount,), jnp.int32).at[sequence[jnp.where(places < fixed, places, passed)]].set(jnp.asarray(sizes, jnp.int32))

    sizes = jnp.where(number % 4 == 0, named(crowded, number // 4), named(ordinary, number - number // 4 - 1))
    mixed = jax.random.permutation(jax.random.fold_in(own, 3), amount)
    donor, receiver = mixed[0:amount // 2 * 2:2], mixed[1:amount // 2 * 2:2]
    slack = jnp.minimum(sizes[donor] - 1, limit - sizes[receiver]) // 2
    slack = jnp.where((donor == sequence[0]) | (receiver == sequence[0]) | (sizes[receiver] == 0), 0, jnp.maximum(slack, 0))
    passed = jax.random.randint(jax.random.fold_in(own, 4), (amount // 2,), 0, 1 << 20) % (slack + 1)
    sizes = sizes.at[donor].add(-passed).at[receiver].add(passed)
    labels = jnp.searchsorted(jnp.cumsum(sizes), jnp.arange(rows * top), side="right").astype(jnp.int32)
    grid = labels.reshape(top, rows).T
    grid = grid[jax.random.permutation(jax.random.fold_in(own, 1), rows)]
    turn = jax.random.randint(jax.random.fold_in(own, 2), (rows, 1), 0, top)
    return jnp.take_along_axis(grid, (jnp.arange(top)[None, :] + turn) % top, axis=1)


def portions_of(amount, total, most, slope, full):
    portions = [(1 << 20) // math.isqrt(rank ** slope) + 1 for rank in range(1, amount + 1)]
    largest = most if full else min(most, max(-(-total // amount), total * portions[0] // sum(portions)))
    least = 1 if total - largest >= amount - 1 else 0
    counts, spare = [largest] + [least] * (amount - 1), total - largest - least * (amount - 1)
    while spare > 0:
        movable = [i for i in range(1, amount) if counts[i] < largest] or [i for i in range(1, amount) if counts[i] < most]
        whole, budget = sum([portions[i] for i in movable]), spare
        for i in movable:
            extra = min(most - counts[i], max(1, budget * portions[i] // whole), spare)
            counts[i] = counts[i] + extra
            spare = spare - extra
    return np.array(counts)


def noise(own_key, dims, spread, limit, cuts=(), kind=jnp.bfloat16):
    values = spread * jax.random.normal(own_key, dims, jnp.float32)
    if cuts:
        values = values * block_levels(own_key, dims, cuts, -0.22, 0.18)
    return jnp.clip(values, -limit, limit).astype(kind)


def setup_inputs(seed: int = 0) -> dict:
    keys = jax.random.split(jax.random.key(seed), 11)
    tokens = noise(keys[0], (TOKENS, D), 1.0, 6.0, ((0, 16), (1, 32)))
    cotangent = noise(keys[1], (TOKENS, D), 0.5, 4.0, ((0, 16), (1, 32)))
    routes_keys = jax.random.split(jax.random.fold_in(keys[2], 1), TOKENS // TOK_GRP)
    routes_turns = jax.random.permutation(jax.random.fold_in(keys[2], 3), TOKENS // TOK_GRP)
    routes = jax.vmap(lambda own, number: shared_out(jax.random.fold_in(keys[2], 2), own, number, TOK_GRP, EXPERTS, TOPK, CAP, 2))(routes_keys, routes_turns).reshape((TOKENS, TOPK))
    gate_weights = jnp.clip(jnp.exp(math.log(2.5) - 3.2227897 * jax.random.uniform(keys[3], (TOKENS, TOPK), jnp.float32) ** block_levels(keys[3], (TOKENS, TOPK), ((0, 16),), -0.2, 0.2)), 0.099609375, 2.5).astype(jnp.bfloat16)
    expert_gate = noise(keys[4], (EXPERTS, D, F), D ** -0.5, 0.09375, ((0, 16), (1, 32)))
    expert_up = noise(keys[5], (EXPERTS, D, F), D ** -0.5, 0.09375, ((0, 16), (1, 32)))
    expert_down = noise(keys[6], (EXPERTS, D, F), F ** -0.5, 0.1875, ((0, 16), (1, 32)))
    shared_gate = noise(keys[7], (D, F), D ** -0.5, 0.09375, ((0, 32),))
    shared_up = noise(keys[8], (D, F), D ** -0.5, 0.09375, ((0, 32),))
    shared_down = noise(keys[9], (D, F), F ** -0.5, 0.1875, ((0, 32),))
    return dict(tokens=tokens, cotangent=cotangent, routes=routes, gate_weights=gate_weights, expert_gate=expert_gate, expert_up=expert_up, expert_down=expert_down, shared_gate=shared_gate, shared_up=shared_up, shared_down=shared_down)


def block_sum(row_block, weight):
    block_width = row_block.shape[1] // N_TP
    partial_value = jnp.einsum('rbd,bdf->brf', row_block.reshape(row_block.shape[0], N_TP, block_width).astype(jnp.float32), weight.reshape(N_TP, block_width, weight.shape[1]).astype(jnp.float32))
    rounded = lax.optimization_barrier(partial_value.astype(jnp.bfloat16))
    return jnp.sum(rounded.astype(jnp.float32), axis=0)


def row_backward(pre_gate, pre_up, back_act, weights):
    sigmoid_gate = jax.nn.sigmoid(pre_gate)
    silu_gate = pre_gate * sigmoid_gate
    activation = silu_gate * pre_up
    act_grad = weights[:, None] * back_act
    grad_up = (act_grad * silu_gate).astype(jnp.bfloat16)
    grad_gate = (act_grad * pre_up * sigmoid_gate * (1.0 + pre_gate * (1.0 - sigmoid_gate))).astype(jnp.bfloat16)
    scaled_act = (weights[:, None] * activation).astype(jnp.bfloat16)
    weight_grad = jnp.sum(activation * back_act, axis=1).astype(jnp.bfloat16)
    return grad_gate, grad_up, scaled_act, weight_grad


def reference(tokens, cotangent, routes, gate_weights, expert_gate, expert_up, expert_down, shared_gate, shared_up, shared_down):
    per_block = TOK_GRP * TOPK
    flat_expert = routes.reshape(N_EP, per_block)
    onehot = (flat_expert[:, :, None] == jnp.arange(EXPERTS, dtype=jnp.int32)[None, None, :]).astype(jnp.int32)
    position = jnp.sum((jnp.cumsum(onehot, axis=1) - onehot) * onehot, axis=2)
    block_id = jnp.arange(N_EP, dtype=jnp.int32)[:, None]
    global_slot = (flat_expert * (N_EP * CAP) + block_id * CAP + position).reshape(-1).astype(jnp.int32)
    owner_row = (jnp.arange(TOKENS * TOPK, dtype=jnp.int32) // TOPK).astype(jnp.int32)
    slots = EXPERTS * N_EP * CAP
    slot_token = jnp.zeros((slots,), jnp.int32).at[global_slot].set(owner_row)
    slot_live = jnp.zeros((slots,), jnp.bfloat16).at[global_slot].set(jnp.ones((TOKENS * TOPK,), jnp.bfloat16))
    slot_weight = jnp.zeros((slots,), jnp.bfloat16).at[global_slot].set(gate_weights.reshape(-1))

    def expert_pass(packed):
        token_ids, live_rows, row_weights, w_gate, w_up, w_down = packed
        in_tokens = tokens[token_ids] * live_rows[:, None]
        in_cotan = cotangent[token_ids] * live_rows[:, None]
        pre_gate = block_sum(in_tokens, w_gate)
        pre_up = block_sum(in_tokens, w_up)
        back_act = block_sum(in_cotan, w_down)
        grad_gate, grad_up, scaled_act, weight_grad = row_backward(pre_gate, pre_up, back_act, row_weights.astype(jnp.float32))
        slot_grad = (jnp.dot(grad_gate, w_gate.T, preferred_element_type=jnp.float32) + jnp.dot(grad_up, w_up.T, preferred_element_type=jnp.float32)).astype(jnp.bfloat16)
        gate_wgrad = jnp.dot(in_tokens.T, grad_gate, preferred_element_type=jnp.float32)
        up_wgrad = jnp.dot(in_tokens.T, grad_up, preferred_element_type=jnp.float32)
        down_wgrad = jnp.dot(in_cotan.T, scaled_act, preferred_element_type=jnp.float32)
        stacked = jnp.stack([gate_wgrad, up_wgrad, down_wgrad])
        squares = jnp.sum(stacked * stacked, axis=1) / D
        return slot_grad, weight_grad, stacked.astype(jnp.bfloat16), squares

    slot_grads, weight_grads, expert_stack, expert_sq = lax.map(expert_pass, (slot_token.reshape(EXPERTS, N_EP * CAP), slot_live.reshape(EXPERTS, N_EP * CAP), slot_weight.reshape(EXPERTS, N_EP * CAP), expert_gate, expert_up, expert_down))
    routed_rows = slot_grads.reshape(slots, D)[global_slot].astype(jnp.float32)
    routed_sum = jnp.sum(routed_rows.reshape(TOKENS, TOPK, D), axis=1)
    gate_grad = weight_grads.reshape(slots)[global_slot].reshape(TOKENS, TOPK)

    def shared_pass(packed):
        block_tokens, block_cotan = packed
        pre_gate = block_sum(block_tokens, shared_gate)
        pre_up = block_sum(block_tokens, shared_up)
        back_act = block_sum(block_cotan, shared_down)
        grad_gate, grad_up, scaled_act, weight_grad = row_backward(pre_gate, pre_up, back_act, jnp.ones((TOK_GRP,), jnp.float32))
        shared_part = jnp.dot(grad_gate, shared_gate.T, preferred_element_type=jnp.float32) + jnp.dot(grad_up, shared_up.T, preferred_element_type=jnp.float32)
        grads = jnp.stack([jnp.dot(block_tokens.T, grad_gate, preferred_element_type=jnp.float32), jnp.dot(block_tokens.T, grad_up, preferred_element_type=jnp.float32), jnp.dot(block_cotan.T, scaled_act, preferred_element_type=jnp.float32)])
        return shared_part, grads

    shared_parts, shared_blocks = lax.map(shared_pass, (tokens.reshape(N_EP, TOK_GRP, D), cotangent.reshape(N_EP, TOK_GRP, D)))
    token_grad = (routed_sum + shared_parts.reshape(TOKENS, D)).astype(jnp.bfloat16)
    shared_grads = jnp.sum(shared_blocks, axis=0)
    shared_norms = jnp.sum(shared_grads * shared_grads, axis=1) / D
    expert_grads = jnp.transpose(expert_stack, (1, 0, 2, 3))
    expert_norms = jnp.transpose(expert_sq, (1, 0, 2))
    return token_grad, gate_grad, expert_grads, shared_grads, expert_norms, shared_norms
```

```python
import jax
import jax.numpy as jnp
from jax import lax
from jax.sharding import PartitionSpec as P

BF = jnp.bfloat16
F32 = jnp.float32


def mm(a, b, dims=((1,), (0,)), precision=None):
    return lax.dot_general(a, b, (dims, ((), ())), precision=precision, preferred_element_type=F32)


def hot(a, b):
    return (a == b).astype(BF)


def row_backward(summed, weights):
    hidden = summed.shape[1] // 3
    pre_gate = summed[:, :hidden]
    pre_up = summed[:, hidden : 2 * hidden]
    back_act = summed[:, 2 * hidden :]
    sigmoid_gate = jax.nn.sigmoid(pre_gate)
    silu_gate = pre_gate * sigmoid_gate
    activation = silu_gate * pre_up
    act_grad = weights * back_act
    grad_up = (act_grad * silu_gate).astype(BF)
    grad_gate = (act_grad * pre_up * sigmoid_gate * (1.0 + pre_gate * (1.0 - sigmoid_gate))).astype(BF)
    scaled_act = (weights * activation).astype(BF)
    weight_grad = jnp.sum(activation * back_act, axis=1, keepdims=True).astype(BF)
    return grad_gate, grad_up, scaled_act, weight_grad


def body(tokens, cotangent, routes, gate_weights, e_gate, e_up, e_down, s_gate, s_up, s_down):
    n_ep, n_tp = lax.axis_size("ep"), lax.axis_size("tp")
    nz = n_tp // 2
    rows, width = tokens.shape
    top = routes.shape[1]
    le, _, hidden = e_gate.shape
    experts = le * n_ep
    cap = 3 * rows * top // (2 * experts)
    ls = le * cap
    bl = (ls + 8) // 8 * 8
    slots = n_ep * ls
    total = slots + rows
    half = total // 2
    piece = total // n_tp
    tp = lax.axis_index("tp")
    z, c = tp // 2, tp % 2
    cw = [(i, (i + 2) % n_tp) for i in range(n_tp)]
    ccw = [(i, (i - 2) % n_tp) for i in range(n_tp)]
    swap = [(i, i ^ 1) for i in range(n_tp)]

    ids = jnp.arange(experts, dtype=jnp.int32)
    on = [hot(routes[:, k : k + 1], ids[None, :]) for k in range(top)]
    tri = (jnp.arange(rows)[:, None] > jnp.arange(rows)[None, :]).astype(BF)
    before = mm(tri, sum(on))
    dest, within = [], []
    for k in range(top):
        pos = jnp.sum(on[k].astype(F32) * before, axis=1).astype(jnp.int32)
        dest.append(routes[:, k] // le)
        within.append(routes[:, k] % le * cap + pos)
    blk = jnp.arange(n_ep * bl, dtype=jnp.int32)
    spread = sum(hot(blk[:, None], (dest[k] * bl + within[k])[None, :]) for k in range(top))
    tail = hot(blk[:, None], (jnp.arange(n_ep, dtype=jnp.int32) * bl + ls)[None, :])
    groups = jnp.arange(n_ep, dtype=jnp.int32)
    lanes = jnp.arange(2 * width, dtype=jnp.int32)
    w_block = sum(
        mm(hot(groups[:, None], dest[k][None, :]) * gate_weights[:, k][None, :], hot(within[k][:, None], lanes[None, :]))
        for k in range(top)
    ).astype(BF)
    both = jnp.concatenate([tokens, cotangent], axis=1)
    sent = mm(jnp.concatenate([spread, tail], 1), jnp.concatenate([both, w_block], 0)).astype(BF)
    got = lax.all_to_all(sent.reshape(n_ep, bl, 2 * width), "ep", 0, 0, tiled=True)

    r = jnp.arange(total, dtype=jnp.int32)
    place = piece * (2 * ((z + r % half // piece) % nz) + (c ^ (r // half))) + r % piece
    kind = jnp.where(place < slots, place % ls // cap, le)
    src = jnp.where(place < slots, place // ls * bl + place % ls, n_ep * bl + place - slots)
    pick = hot(src[:, None], jnp.arange(n_ep * bl + rows, dtype=jnp.int32)[None, :])
    mine = mm(pick, jnp.concatenate([got.reshape(n_ep * bl, 2 * width), both], 0)).astype(BF)
    masks = [(kind == e)[:, None] for e in range(le + 1)]
    x_rows = jnp.concatenate([jnp.where(m, mine[:, :width], 0) for m in masks], 1)
    g_rows = jnp.concatenate([jnp.where(m, mine[:, width:], 0) for m in masks], 1)
    w_gate = jnp.concatenate([e_gate.reshape(le * width, hidden), s_gate], 0)
    w_up = jnp.concatenate([e_up.reshape(le * width, hidden), s_up], 0)
    w_down = jnp.concatenate([e_down.reshape(le * width, hidden), s_down], 0)
    part = jnp.concatenate([mm(x_rows, w_gate), mm(x_rows, w_up), mm(g_rows, w_down)], 1).astype(BF)
    own = part[:half].reshape(nz, piece, 3 * hidden)
    other = lax.ppermute(part[half:], "tp", swap).reshape(nz, piece, 3 * hidden)

    def local(j):
        return own[j % nz].astype(F32) + other[j % nz].astype(F32)

    hops, back_hops = nz // 2, nz - nz // 2 - 1
    right, left = local(hops).astype(BF), local(-back_hops).astype(BF)
    for t in range(hops):
        right = lax.ppermute(right, "tp", cw)
        if t < hops - 1:
            right = (right.astype(F32) + local(hops - 1 - t)).astype(BF)
        if t < back_hops:
            left = lax.ppermute(left, "tp", ccw)
        if t < back_hops - 1:
            left = (left.astype(F32) + local(t + 1 - back_hops)).astype(BF)
    summed = right.astype(F32) + left.astype(F32) + local(0)

    q = tp * piece + jnp.arange(piece, dtype=jnp.int32)
    w_rows = mm(hot((q // ls)[:, None], groups[None, :]), got[:, ls, :])
    own_w = jnp.sum(jnp.where((q % ls)[:, None] == lanes[None, :], w_rows, 0.0), axis=1)
    own_w = jnp.where(q < slots, own_w, 1.0)[:, None]
    gg, gu, sa, wg = row_backward(summed, own_w)
    block = jnp.concatenate([gg, gu, sa, jnp.broadcast_to(wg, (piece, 128))], 1)

    ring = [None] * nz
    ring[0] = right = left = block
    for t in range(1, hops + 1):
        right = lax.ppermute(right, "tp", cw)
        ring[-t % nz] = right
        if t <= back_hops:
            left = lax.ppermute(left, "tp", ccw)
            ring[t] = left
    kept = jnp.concatenate(ring, 0)
    grads = jnp.concatenate([kept, lax.ppermute(kept, "tp", swap)], 0)
    gg, gu, sa, wg = grads[:, :hidden], grads[:, hidden : 2 * hidden], grads[:, 2 * hidden : 3 * hidden], grads[:, 3 * hidden :]

    first = ((0,), (0,))
    stack = jnp.stack(
        [mm(a[:, : le * width], b, first).reshape(le, width, hidden) for a, b in ((x_rows, gg), (x_rows, gu), (g_rows, sa))]
    )
    e_sq = jnp.sum(stack * stack, axis=2)
    piece_sq = e_sq.reshape(n_tp, -1)
    piece_sq = jnp.sum(lax.all_to_all(piece_sq, "tp", 0, 0, tiled=True), axis=0)

    last = ((1,), (1,))
    slot = mm(gg, w_gate, last) + mm(gu, w_up, last)
    slot = sum(jnp.where(m, slot[:, e * width : (e + 1) * width], 0.0) for e, m in enumerate(masks))
    routed = pick[:, : n_ep * bl]
    lane1 = jnp.arange(width, dtype=jnp.int32)
    wg_block = mm(
        hot(groups[:, None], jnp.where(place < slots, place // ls, -1)[None, :]) * wg[:, 0][None, :],
        hot((place % ls)[:, None], lane1[None, :]),
    ).astype(BF)
    back = mm(routed, slot.astype(BF), first) + mm(tail, wg_block)
    shared_part = mm(pick[:, n_ep * bl :].astype(F32), slot, first, lax.Precision.HIGHEST)
    x_sh, g_sh = x_rows[:, le * width :], g_rows[:, le * width :]
    sh = jnp.stack([mm(gg, x_sh, first), mm(gu, x_sh, first), mm(sa, g_sh, first)]).astype(BF)
    cols = hidden // n_ep
    sh = jnp.moveaxis(sh.reshape(3, n_ep, cols, width), 1, 0).reshape(n_ep, 3 * cols, width)
    out = jnp.concatenate([back.astype(BF).reshape(n_ep, bl, width), sh], axis=1)
    home = lax.all_to_all(out, "ep", 0, 0, tiled=True)
    rows_home = home[:, :bl].reshape(n_ep * bl, width)
    token_grad = (mm(spread, rows_home, first) + shared_part).astype(BF)
    wg_home = home[:, ls]
    gate_grad = []
    for k in range(top):
        line = mm(hot(dest[k][:, None], groups[None, :]), wg_home)
        gate_grad.append(jnp.sum(jnp.where(within[k][:, None] == lane1[None, :], line, 0.0), axis=1))
    gate_grad = jnp.stack(gate_grad, 1).astype(BF)
    shared = jnp.sum(home[:, bl:].astype(F32), axis=0).reshape(3, cols, width)
    s_sq = jnp.sum(shared * shared, axis=2).reshape(-1)
    line = jnp.concatenate([piece_sq, s_sq])
    lines = lax.all_to_all(jnp.broadcast_to(line[None], (n_tp, line.size)), "tp", 0, 0, tiled=True)
    scale = 1.0 / (width * n_tp)
    n_e = piece_sq.size
    return (
        token_grad,
        gate_grad,
        stack.astype(BF),
        jnp.swapaxes(shared, 1, 2),
        lines[:, :n_e].reshape(3, le, hidden) * scale,
        jnp.sum(lines[:, n_e:], axis=0).reshape(3, cols) * scale,
    )


def solution(mesh):
    return jax.shard_map(
        body,
        mesh=mesh,
        in_specs=(
            P("ep", "tp"),
            P("ep", "tp"),
            P("ep", None),
            P("ep", None),
            P("ep", "tp", None),
            P("ep", "tp", None),
            P("ep", "tp", None),
            P("tp", None),
            P("tp", None),
            P("tp", None),
        ),
        out_specs=(
            P("ep", "tp"),
            P("ep", None),
            P(None, "ep", "tp", None),
            P(None, "tp", "ep"),
            P(None, "ep", None),
            P(None, "ep"),
        ),
        check_vma=False,
    )
```

```python
import jax
import jax.numpy as jnp
from jax import lax
from jax.experimental import pallas as pl
from jax.experimental.pallas import tpu as pltpu
from jax.sharding import PartitionSpec as P

BF = jnp.bfloat16
F32 = jnp.float32
VM = pl.BlockSpec(memory_space=pltpu.VMEM)


def mm(a, b, dims=((1,), (0,))):
    return lax.dot_general(a, b, (dims, ((), ())), preferred_element_type=F32)


NT = ((1,), (1,))


def hot(a, b):
    return (a == b).astype(BF)


def call(kernel, outs, *args):
    return pl.pallas_call(
        kernel,
        out_shape=[jax.ShapeDtypeStruct(s, d) for s, d in outs],
        in_specs=[VM] * len(args),
        out_specs=[VM] * len(outs),
    )(*args)


def project(pick, got, both, kind, eg, eu, ed, sg, su, sd, own_r, own_l, out_r, out_l, mine_ref):
    le, width, hidden = eg.shape
    nb = got.shape[0]
    mine = mm(pick[:, :nb], got[...]) + mm(pick[:, nb:], both[...])
    mine_ref[...] = mine.astype(BF)
    kd = kind[...]
    part = [jnp.where(kd == e, mine, 0.0).astype(BF) for e in range(le + 1)]
    x = jnp.concatenate([p[:, :width] for p in part[:le]], 1)
    g = jnp.concatenate([p[:, width:] for p in part[:le]], 1)
    nr, nl = own_r.shape[0], own_l.shape[0]
    half = nr + nl
    todo = ((x, part[le][:, :width], eg, sg), (x, part[le][:, :width], eu, su), (g, part[le][:, width:], ed, sd))
    for t, (xe, xs, we, ws) in enumerate(todo):
        cols = slice(t * hidden, (t + 1) * hidden)
        p = mm(xe, we[...].reshape(le * width, hidden)) + mm(xs, ws[...])
        own_r[:, cols] = p[:nr]
        own_l[:, cols] = p[nr:half]
        out_r[:, cols] = p[half : half + nr].astype(BF)
        out_l[:, cols] = p[half + nr :].astype(BF)


def shared_grads(kept, other, xt, gt, out):
    half = kept.shape[0]
    n_ep, rows, width = out.shape
    cols = rows // 3
    hidden = cols * n_ep
    for t, lhs in enumerate((xt, xt, gt)):
        part = slice(t * hidden, (t + 1) * hidden)
        r = mm(lhs[:, :half], kept[:, part]) + mm(lhs[:, half:], other[:, part])
        out[:, t * cols : (t + 1) * cols, :] = r.T.astype(BF).reshape(n_ep, cols, width)


def expert_grads(kept, other, xt, gt, eg, eu, sg, su, kind, pick_t, tail_t, lane_hot, stack, sq, back, shared):
    le, width, hidden = eg.shape
    half = kept.shape[0]
    nb = back.shape[0]
    slots = []
    for h, src in enumerate((kept, other)):
        gg, gu = src[:, :hidden], src[:, hidden : 2 * hidden]
        se = mm(gg, eg[...].reshape(le * width, hidden), NT) + mm(gu, eu[...].reshape(le * width, hidden), NT)
        ss = mm(gg, sg[...], NT) + mm(gu, su[...], NT)
        kd = kind[h * half : (h + 1) * half, :]
        s = jnp.where(kd == le, ss, 0.0)
        for e in range(le):
            s = s + jnp.where(kd == e, se[:, e * width : (e + 1) * width], 0.0)
        slots.append(s)
    slot = jnp.concatenate(slots, 0)
    hi = slot.astype(BF)
    rest = slot - hi.astype(F32)
    mid = rest.astype(BF)
    low = (rest - mid.astype(F32)).astype(BF)
    wg = jnp.concatenate([kept[:, 3 * hidden :], other[:, 3 * hidden :]], 0).astype(F32)
    wg = (wg * lane_hot[...].astype(F32)).astype(BF)
    back[...] = (mm(pick_t[:nb, :], hi) + mm(tail_t[...], wg)).astype(BF)
    ps = pick_t[nb:, :]
    shared[...] = mm(ps, hi) + mm(ps, mid) + mm(ps, low)
    for t, lhs in enumerate((xt, xt, gt)):
        part = slice(t * hidden, (t + 1) * hidden)
        r = mm(lhs[:, :half], kept[:, part]) + mm(lhs[:, half:], other[:, part])
        r = r.reshape(le, width, hidden)
        stack[t] = r.astype(BF)
        sq[t] = jnp.sum(r * r, axis=1)


def row_backward(summed, weights):
    hidden = summed.shape[1] // 3
    pre_gate = summed[:, :hidden]
    pre_up = summed[:, hidden : 2 * hidden]
    back_act = summed[:, 2 * hidden :]
    sigmoid_gate = jax.nn.sigmoid(pre_gate)
    silu_gate = pre_gate * sigmoid_gate
    activation = silu_gate * pre_up
    act_grad = weights * back_act
    grad_up = (act_grad * silu_gate).astype(BF)
    grad_gate = (act_grad * pre_up * sigmoid_gate * (1.0 + pre_gate * (1.0 - sigmoid_gate))).astype(BF)
    scaled_act = (weights * activation).astype(BF)
    weight_grad = jnp.sum(activation * back_act, axis=1, keepdims=True).astype(BF)
    return grad_gate, grad_up, scaled_act, weight_grad


def body(tokens, cotangent, routes, gate_weights, e_gate, e_up, e_down, s_gate, s_up, s_down):
    n_ep, n_tp = lax.axis_size("ep"), lax.axis_size("tp")
    nz = n_tp // 2
    rows, width = tokens.shape
    top = routes.shape[1]
    le, _, hidden = e_gate.shape
    experts = le * n_ep
    cap = 3 * rows * top // (2 * experts)
    ls = le * cap
    bl = (ls + 8) // 8 * 8
    slots = n_ep * ls
    total = slots + rows
    half = total // 2
    piece = total // n_tp
    tp = lax.axis_index("tp")
    z, c = tp // 2, tp % 2
    fwd = [(i, (i + 2 - 4 * (i % 2)) % n_tp) for i in range(n_tp)]
    bwd = [(i, (i - 2 + 4 * (i % 2)) % n_tp) for i in range(n_tp)]
    swap = [(i, i ^ 1) for i in range(n_tp)]

    ids = jnp.arange(experts, dtype=jnp.int32)
    on = [hot(routes[:, k : k + 1], ids[None, :]) for k in range(top)]
    tri = (jnp.arange(rows)[:, None] > jnp.arange(rows)[None, :]).astype(BF)
    before = mm(tri, sum(on))
    dest, within = [], []
    for k in range(top):
        pos = jnp.sum(on[k].astype(F32) * before, axis=1).astype(jnp.int32)
        dest.append(routes[:, k] // le)
        within.append(routes[:, k] % le * cap + pos)
    blk = jnp.arange(n_ep * bl, dtype=jnp.int32)
    spread = sum(hot(blk[:, None], (dest[k] * bl + within[k])[None, :]) for k in range(top))
    tail = hot(blk[:, None], (jnp.arange(n_ep, dtype=jnp.int32) * bl + ls)[None, :])
    groups = jnp.arange(n_ep, dtype=jnp.int32)
    lanes = jnp.arange(2 * width, dtype=jnp.int32)
    w_block = sum(
        mm(hot(groups[:, None], dest[k][None, :]) * gate_weights[:, k][None, :], hot(within[k][:, None], lanes[None, :]))
        for k in range(top)
    ).astype(BF)
    both = jnp.concatenate([tokens, cotangent], axis=1)
    sent = mm(jnp.concatenate([spread, tail], 1), jnp.concatenate([both, w_block], 0)).astype(BF)
    got = lax.all_to_all(sent.reshape(n_ep, bl, 2 * width), "ep", 0, 0, tiled=True)

    r = jnp.arange(total, dtype=jnp.int32)
    h = r // half
    turn = (1 - 2 * c) * (1 - 2 * h) * (r % half // piece)
    place = piece * (2 * ((z + turn) % nz) + (c ^ h)) + r % piece
    kind = jnp.where(place < slots, place % ls // cap, le)
    src = jnp.where(place < slots, place // ls * bl + place % ls, n_ep * bl + place - slots)
    column = jnp.arange(n_ep * bl + rows, dtype=jnp.int32)
    pick = hot(src[:, None], column[None, :])
    hops, back_hops = nz // 2, nz - nz // 2 - 1
    nr, nl = (hops + 1) * piece, back_hops * piece
    width3 = 3 * hidden
    own_r, own_l, out_r, out_l, mine = call(
        project,
        [((nr, width3), F32), ((nl, width3), F32), ((nr, width3), BF), ((nl, width3), BF), ((total, 2 * width), BF)],
        pick, got.reshape(n_ep * bl, 2 * width), both, kind[:, None], e_gate, e_up, e_down, s_gate, s_up, s_down,
    )
    oth_r = lax.ppermute(out_r, "tp", swap)
    oth_l = lax.ppermute(out_l, "tp", swap)

    def at_r(j):
        rows_j = slice(j * piece, (j + 1) * piece)
        return own_r[rows_j] + oth_r[rows_j].astype(F32)

    def at_l(j):
        rows_j = slice((back_hops - j) * piece, (back_hops - j + 1) * piece)
        return own_l[rows_j] + oth_l[rows_j].astype(F32)

    right, left = at_r(hops).astype(BF), at_l(back_hops).astype(BF)
    for t in range(hops):
        right = lax.ppermute(right, "tp", fwd)
        if t < hops - 1:
            right = right.astype(F32) + at_r(hops - 1 - t)
            right = right if t == hops - 2 else right.astype(BF)
        if t < back_hops:
            left = lax.ppermute(left, "tp", bwd)
        if t < back_hops - 1:
            left = left.astype(F32) + at_l(back_hops - 1 - t)
            left = left if t == back_hops - 2 else left.astype(BF)
    summed = right.astype(F32) + left.astype(F32) + at_r(0)

    q = tp * piece + jnp.arange(piece, dtype=jnp.int32)
    w_rows = mm(hot((q // ls)[:, None], groups[None, :]), got[:, ls, :])
    own_w = jnp.sum(jnp.where((q % ls)[:, None] == lanes[None, :], w_rows, 0.0), axis=1)
    own_w = jnp.where(q < slots, own_w, 1.0)[:, None]
    gg, gu, sa, wg = row_backward(summed, own_w)
    block = jnp.concatenate([gg, gu, sa, jnp.broadcast_to(wg, (piece, 128))], 1)

    ring = [None] * nz
    ring[0] = right = left = block
    for t in range(1, hops + 1):
        right = lax.ppermute(right, "tp", fwd)
        ring[-t % nz] = right
        if t <= back_hops:
            left = lax.ppermute(left, "tp", bwd)
            ring[t] = left
    kept = jnp.concatenate(ring, 0)
    other = lax.ppermute(kept, "tp", swap)

    kind_row = kind[None, :]
    mine_t = mine.T
    x_t = [jnp.where(kind_row == e, mine_t[:width], 0) for e in range(le + 1)]
    g_t = [jnp.where(kind_row == e, mine_t[width:], 0) for e in range(le + 1)]
    cols = hidden // n_ep
    (sh,) = call(shared_grads, [((n_ep, 3 * cols, width), BF)], kept, other, x_t[le], g_t[le])
    sh_home = lax.all_to_all(sh, "ep", 0, 0, tiled=True)

    lane1 = jnp.arange(width, dtype=jnp.int32)
    pick_t = hot(column[:, None], src[None, :])
    tail_t = hot(blk[:, None], jnp.where(place < slots, place // ls * bl + ls, -1)[None, :])
    lane_hot = hot((place % ls)[:, None], lane1[None, :])
    stack, e_sq, back, shared_part = call(
        expert_grads,
        [((3, le, width, hidden), BF), ((3, le, hidden), F32), ((n_ep * bl, width), BF), ((rows, width), F32)],
        kept, other, jnp.concatenate(x_t[:le], 0), jnp.concatenate(g_t[:le], 0),
        e_gate, e_up, s_gate, s_up, kind[:, None], pick_t, tail_t, lane_hot,
    )
    piece_sq = jnp.sum(lax.all_to_all(e_sq.reshape(n_tp, -1), "tp", 0, 0, tiled=True), axis=0)
    home = lax.all_to_all(back.reshape(n_ep, bl, width), "ep", 0, 0, tiled=True)
    rows_home = home.reshape(n_ep * bl, width)
    token_grad = (mm(spread, rows_home, ((0,), (0,))) + shared_part).astype(BF)
    wg_home = home[:, ls]
    gate_grad = []
    for k in range(top):
        line = mm(hot(dest[k][:, None], groups[None, :]), wg_home)
        gate_grad.append(jnp.sum(jnp.where(within[k][:, None] == lane1[None, :], line, 0.0), axis=1))
    gate_grad = jnp.stack(gate_grad, 1).astype(BF)
    shared = jnp.sum(sh_home.astype(F32), axis=0).reshape(3, cols, width)
    s_sq = jnp.sum(shared * shared, axis=2).reshape(-1)
    line = jnp.concatenate([piece_sq, s_sq])
    lines = lax.all_to_all(jnp.broadcast_to(line[None], (n_tp, line.size)), "tp", 0, 0, tiled=True)
    scale = 1.0 / (width * n_tp)
    n_e = piece_sq.size
    return (
        token_grad,
        gate_grad,
        stack,
        jnp.swapaxes(shared, 1, 2),
        lines[:, :n_e].reshape(3, le, hidden) * scale,
        jnp.sum(lines[:, n_e:], axis=0).reshape(3, cols) * scale,
    )


def solution(mesh):
    return jax.shard_map(
        body,
        mesh=mesh,
        in_specs=(
            P("ep", "tp"),
            P("ep", "tp"),
            P("ep", None),
            P("ep", None),
            P("ep", "tp", None),
            P("ep", "tp", None),
            P("ep", "tp", None),
            P("tp", None),
            P("tp", None),
            P("tp", None),
        ),
        out_specs=(
            P("ep", "tp"),
            P("ep", None),
            P(None, "ep", "tp", None),
            P(None, "tp", "ep"),
            P(None, "ep", None),
            P(None, "ep"),
        ),
        check_vma=False,
    )
```

```python
import functools

import jax
import jax.numpy as jnp
from jax import lax
from jax.experimental import pallas as pl
from jax.experimental.pallas import tpu as pltpu
from jax.sharding import PartitionSpec as P


BF = jnp.bfloat16
F32 = jnp.float32
VM = pl.BlockSpec(memory_space=pltpu.VMEM)


def mm(a, b, dims=((1,), (0,))):
    return lax.dot_general(a, b, (dims, ((), ())), preferred_element_type=F32)


NT = ((1,), (1,))


def hot(a, b):
    return (a == b).astype(BF)


def call(kernel, outs, *args, smem=0, rest=0):
    first = [pl.BlockSpec(memory_space=pltpu.SMEM)] * smem
    last = [pl.BlockSpec(memory_space=pl.ANY)] * rest
    return pl.pallas_call(
        kernel,
        out_shape=[jax.ShapeDtypeStruct(s, d) for s, d in outs],
        in_specs=first + [VM] * (len(args) - smem - rest) + last,
        out_specs=[VM] * len(outs),
    )(*args)


def quotient(n, by, top):
    shift = 0
    while (1 << shift) < by * top:
        shift += 1
    factor = -(-(1 << shift) // by)
    assert factor * top < 2**31
    return lax.shift_right_logical(n * factor, jnp.int32(shift))


def ring_rows(r, z, c, sizes):
    nz, piece, ls, cap, bl, slots = sizes
    half = nz * piece
    h = (r >= half).astype(jnp.int32)
    inner = r - half * h
    j = quotient(inner, piece, half)
    turn = (1 - 2 * c) * (1 - 2 * h) * j
    place = piece * (2 * ((z + turn) & (nz - 1)) + jnp.abs(c - h)) + inner - piece * j
    block = quotient(place, ls, 2 * half)
    within = place - ls * block
    routed = place < slots
    expert = jnp.where(routed, quotient(within, cap, ls), ls // cap)
    src = jnp.where(routed, block * bl + within, slots // ls * bl + place - slots)
    return src, expert, jnp.where(routed, block, -1), within


def along(n, dim):
    return lax.broadcasted_iota(jnp.int32, (n, 1) if dim == 0 else (1, n), dim)


def one_hot(a, b):
    return jnp.where(a == b, 1.0, 0.0).astype(BF)


def project(sizes, pos, got, both, eg, eu, ed, sg, su, sd, own_r, own_l, out_r, out_l, xt_ref, gt_ref, xs_ref, gs_ref):
    le, width, hidden = eg.shape
    nb, rows = got.shape[0], both.shape[0]
    nr, nl = own_r.shape[0], own_l.shape[0]
    half = nr + nl
    z, c = pos[0], pos[1]
    src, kd, _, _ = ring_rows(along(2 * half, 0), z, c, sizes)
    cols = lax.broadcasted_iota(jnp.int32, (2 * half, nb), 1)
    mine = mm(one_hot(src, cols), got[...])
    mine = mine + mm(one_hot(src - nb, lax.broadcasted_iota(jnp.int32, (2 * half, rows), 1)), both[...])
    part = [jnp.where(kd == e, mine, 0.0).astype(BF) for e in range(le + 1)]
    x = jnp.concatenate([p[:, :width] for p in part[:le]], 1)
    g = jnp.concatenate([p[:, width:] for p in part[:le]], 1)
    todo = ((x, part[le][:, :width], eg, sg), (x, part[le][:, :width], eu, su), (g, part[le][:, width:], ed, sd))
    for t, (xe, xs, we, ws) in enumerate(todo):
        cut = slice(t * hidden, (t + 1) * hidden)
        p = mm(xe, we[...].reshape(le * width, hidden)) + mm(xs, ws[...])
        own_r[:, cut] = p[:nr]
        own_l[:, cut] = p[nr:half]
        out_r[:, cut] = p[half : half + nr].astype(BF)
        out_l[:, cut] = p[half + nr :].astype(BF)
    _, kr, _, _ = ring_rows(along(2 * half, 1), z, c, sizes)
    mine_t = mine.T
    for e in range(le + 1):
        both_t = jnp.where(kr == e, mine_t, 0.0).astype(BF)
        to_x, to_g, at = (xt_ref, gt_ref, e * width) if e < le else (xs_ref, gs_ref, 0)
        to_x[at : at + width, :] = both_t[:width]
        to_g[at : at + width, :] = both_t[width:]


def over_rows(lhs, parts, cut):
    at, out = 0, None
    for p in parts:
        n = p.shape[0]
        r = mm(lhs[:, at : at + n], p[:, cut])
        out = r if out is None else out + r
        at += n
    return out


def expert_grads(kept, other, xt, gt, stack, sq):
    _, le, width, hidden = stack.shape
    for t, lhs in enumerate((xt, xt, gt)):
        r = over_rows(lhs, (kept, other), slice(t * hidden, (t + 1) * hidden)).reshape(le, width, hidden)
        stack[t] = r.astype(BF)
        sq[t] = jnp.sum(r * r, axis=1)


def row_grads(sizes, pos, kept, other, eg, eu, sg, su, xs, gs, after, out, shared):
    le, width, hidden = eg.shape
    ls, bl = sizes[2], sizes[4]
    n_ep, rows = out.shape[0], shared.shape[0]
    nb = n_ep * bl
    cols = hidden // n_ep
    for t, lhs in enumerate((xs, xs, gs)):
        r = over_rows(lhs, (kept, other), slice(t * hidden, (t + 1) * hidden))
        out[:, t * cols : (t + 1) * cols, :] = r.T.astype(BF).reshape(n_ep, cols, width)
    total = 2 * sizes[0] * sizes[1]
    z, c = pos[0], pos[1]
    _, kd, _, within = ring_rows(along(total, 0), z, c, sizes)
    slots, wg, at = [], [], 0
    for src in (kept, other):
        n = src.shape[0]
        gg, gu = src[:, :hidden], src[:, hidden : 2 * hidden]
        se = mm(gg, eg[...].reshape(le * width, hidden), NT) + mm(gu, eu[...].reshape(le * width, hidden), NT)
        ss = mm(gg, sg[...], NT) + mm(gu, su[...], NT)
        k = kd[at : at + n]
        s = jnp.where(k == le, ss, 0.0)
        for e in range(le):
            s = s + jnp.where(k == e, se[:, e * width : (e + 1) * width], 0.0)
        slots.append(s)
        lanes = lax.broadcasted_iota(jnp.int32, (n, width), 1)
        wg.append(jnp.where(within[at : at + n] == lanes, src[:, 3 * hidden :].astype(F32), 0.0))
        at += n
    slot = jnp.concatenate(slots, 0)
    hi = slot.astype(BF)
    rest = slot - hi.astype(F32)
    mid = rest.astype(BF)
    low = (rest - mid.astype(F32)).astype(BF)
    src_r, _, block, _ = ring_rows(along(total, 1), z, c, sizes)
    lines = lax.broadcasted_iota(jnp.int32, (nb, total), 0)
    to_slot = one_hot(lines, src_r)
    to_tail = one_hot(lines, jnp.where(block >= 0, block * bl + ls, -1))
    back = mm(to_slot, hi) + mm(to_tail, jnp.concatenate(wg, 0).astype(BF))
    out[:, 3 * cols :, :] = back.reshape(n_ep, bl, width).astype(BF)
    ps = one_hot(lax.broadcasted_iota(jnp.int32, (rows, total), 0) + nb, src_r)
    shared[...] = mm(ps, hi) + mm(ps, mid) + mm(ps, low)


def row_backward(summed, weights):
    hidden = summed.shape[1] // 3
    pre_gate = summed[:, :hidden]
    pre_up = summed[:, hidden : 2 * hidden]
    back_act = summed[:, 2 * hidden :]
    sigmoid_gate = jax.nn.sigmoid(pre_gate)
    silu_gate = pre_gate * sigmoid_gate
    activation = silu_gate * pre_up
    act_grad = weights * back_act
    grad_up = (act_grad * silu_gate).astype(BF)
    grad_gate = (act_grad * pre_up * sigmoid_gate * (1.0 + pre_gate * (1.0 - sigmoid_gate))).astype(BF)
    scaled_act = (weights * activation).astype(BF)
    weight_grad = jnp.sum(activation * back_act, axis=1, keepdims=True).astype(BF)
    return grad_gate, grad_up, scaled_act, weight_grad


def body(tokens, cotangent, routes, gate_weights, e_gate, e_up, e_down, s_gate, s_up, s_down):
    n_ep, n_tp = lax.axis_size("ep"), lax.axis_size("tp")
    nz = n_tp // 2
    rows, width = tokens.shape
    top = routes.shape[1]
    le, _, hidden = e_gate.shape
    experts = le * n_ep
    cap = 3 * rows * top // (2 * experts)
    ls = le * cap
    bl = (ls + 8) // 8 * 8
    slots = n_ep * ls
    total = slots + rows
    piece = total // n_tp
    tp = lax.axis_index("tp")
    z, c = tp // 2, tp % 2
    fwd = [(i, (i + 2 - 4 * (i % 2)) % n_tp) for i in range(n_tp)]
    bwd = [(i, (i - 2 + 4 * (i % 2)) % n_tp) for i in range(n_tp)]
    swap = [(i, i ^ 1) for i in range(n_tp)]

    ids = jnp.arange(experts, dtype=jnp.int32)
    on = [hot(routes[:, k : k + 1], ids[None, :]) for k in range(top)]
    tri = (jnp.arange(rows)[:, None] > jnp.arange(rows)[None, :]).astype(BF)
    before = mm(tri, sum(on))
    dest, within = [], []
    for k in range(top):
        pos = jnp.sum(on[k].astype(F32) * before, axis=1).astype(jnp.int32)
        dest.append(routes[:, k] // le)
        within.append(routes[:, k] % le * cap + pos)
    blk = jnp.arange(n_ep * bl, dtype=jnp.int32)
    spread = sum(hot(blk[:, None], (dest[k] * bl + within[k])[None, :]) for k in range(top))
    tail = hot(blk[:, None], (jnp.arange(n_ep, dtype=jnp.int32) * bl + ls)[None, :])
    groups = jnp.arange(n_ep, dtype=jnp.int32)
    lanes = jnp.arange(2 * width, dtype=jnp.int32)
    w_block = sum(
        mm(hot(groups[:, None], dest[k][None, :]) * gate_weights[:, k][None, :], hot(within[k][:, None], lanes[None, :]))
        for k in range(top)
    ).astype(BF)
    both = jnp.concatenate([tokens, cotangent], axis=1)
    sent = mm(jnp.concatenate([spread, tail], 1), jnp.concatenate([both, w_block], 0)).astype(BF)
    got = lax.all_to_all(sent.reshape(n_ep, bl, 2 * width), "ep", 0, 0, tiled=True)

    sizes = (nz, piece, ls, cap, bl, slots)
    pos = jnp.stack([z, c]).astype(jnp.int32)
    hops, back_hops = nz // 2, nz - nz // 2 - 1
    nr, nl = (hops + 1) * piece, back_hops * piece
    width3 = 3 * hidden
    own_r, own_l, out_r, out_l, xt, gt, xs, gs = call(
        functools.partial(project, sizes),
        [((nr, width3), F32), ((nl, width3), F32), ((nr, width3), BF), ((nl, width3), BF)]
        + [((le * width, total), BF)] * 2
        + [((width, total), BF)] * 2,
        pos, got.reshape(n_ep * bl, 2 * width), both, e_gate, e_up, e_down, s_gate, s_up, s_down, smem=1,
    )
    oth_r = lax.ppermute(out_r, "tp", swap)
    oth_l = lax.ppermute(out_l, "tp", swap)

    def at_r(j):
        rows_j = slice(j * piece, (j + 1) * piece)
        return own_r[rows_j] + oth_r[rows_j].astype(F32)

    def at_l(j):
        rows_j = slice((back_hops - j) * piece, (back_hops - j + 1) * piece)
        return own_l[rows_j] + oth_l[rows_j].astype(F32)

    right, left = at_r(hops).astype(BF), at_l(back_hops).astype(BF)
    for t in range(hops):
        right = lax.ppermute(right, "tp", fwd)
        if t < hops - 1:
            right = right.astype(F32) + at_r(hops - 1 - t)
            right = right if t == hops - 2 else right.astype(BF)
        if t < back_hops:
            left = lax.ppermute(left, "tp", bwd)
        if t < back_hops - 1:
            left = left.astype(F32) + at_l(back_hops - 1 - t)
            left = left if t == back_hops - 2 else left.astype(BF)
    summed = right.astype(F32) + left.astype(F32) + at_r(0)

    q = tp * piece + jnp.arange(piece, dtype=jnp.int32)
    w_rows = mm(hot((q // ls)[:, None], groups[None, :]), got[:, ls, :])
    own_w = jnp.sum(jnp.where((q % ls)[:, None] == lanes[None, :], w_rows, 0.0), axis=1)
    own_w = jnp.where(q < slots, own_w, 1.0)[:, None]
    gg, gu, sa, wg = row_backward(summed, own_w)
    block = jnp.concatenate([gg, gu, sa, jnp.broadcast_to(wg, (piece, 128))], 1)

    ring = [None] * nz
    ring[0] = right = left = block
    for t in range(1, hops + 1):
        right = lax.ppermute(right, "tp", fwd)
        ring[-t % nz] = right
        if t <= back_hops:
            left = lax.ppermute(left, "tp", bwd)
            ring[t] = left
    kept = jnp.concatenate(ring, 0)
    grads = (kept, lax.ppermute(kept, "tp", swap))

    cols = hidden // n_ep
    stack, e_sq = call(
        expert_grads, [((3, le, width, hidden), BF), ((3, le, hidden), F32)], *grads, xt, gt
    )
    piece_sq = lax.all_to_all(e_sq.reshape(n_tp, -1), "tp", 0, 0, tiled=True)
    piece_sq = jnp.sum(piece_sq, axis=0)
    out, shared_part = call(
        functools.partial(row_grads, sizes),
        [((n_ep, 3 * cols + bl, width), BF), ((rows, width), F32)],
        pos, *grads, e_gate, e_up, s_gate, s_up, xs, gs, e_sq, smem=1, rest=1,
    )
    home = lax.all_to_all(out, "ep", 0, 0, tiled=True)
    sh_home, home = home[:, : 3 * cols], home[:, 3 * cols :]
    lane1 = jnp.arange(width, dtype=jnp.int32)
    shared = jnp.sum(sh_home.astype(F32), axis=0).reshape(3, cols, width)
    s_sq = jnp.sum(shared * shared, axis=2).reshape(-1)
    line = jnp.concatenate([piece_sq, s_sq])
    home, line = lax.optimization_barrier((home, line))
    lines = lax.all_to_all(jnp.broadcast_to(line[None], (n_tp, line.size)), "tp", 0, 0, tiled=True)
    rows_home = home.reshape(n_ep * bl, width)
    token_grad = (mm(spread, rows_home, ((0,), (0,))) + shared_part).astype(BF)
    wg_home = home[:, ls]
    gate_grad = []
    for k in range(top):
        line = mm(hot(dest[k][:, None], groups[None, :]), wg_home)
        gate_grad.append(jnp.sum(jnp.where(within[k][:, None] == lane1[None, :], line, 0.0), axis=1))
    gate_grad = jnp.stack(gate_grad, 1).astype(BF)
    scale = 1.0 / (width * n_tp)
    n_e = piece_sq.size
    return (
        token_grad,
        gate_grad,
        stack,
        jnp.swapaxes(shared, 1, 2),
        lines[:, :n_e].reshape(3, le, hidden) * scale,
        jnp.sum(lines[:, n_e:], axis=0).reshape(3, cols) * scale,
    )


def solution(mesh):
    return jax.shard_map(
        body,
        mesh=mesh,
        in_specs=(
            P("ep", "tp"),
            P("ep", "tp"),
            P("ep", None),
            P("ep", None),
            P("ep", "tp", None),
            P("ep", "tp", None),
            P("ep", "tp", None),
            P("tp", None),
            P("tp", None),
            P("tp", None),
        ),
        out_specs=(
            P("ep", "tp"),
            P("ep", None),
            P(None, "ep", "tp", None),
            P(None, "tp", "ep"),
            P(None, "ep", None),
            P(None, "ep"),
        ),
        check_vma=False,
    )
```

```python
import functools

import jax
import jax.numpy as jnp
from jax import lax
from jax.experimental import pallas as pl
from jax.experimental.pallas import tpu as pltpu
from jax.sharding import PartitionSpec as P


BF = jnp.bfloat16
F32 = jnp.float32
VM = pl.BlockSpec(memory_space=pltpu.VMEM)


def mm(a, b, dims=((1,), (0,))):
    return lax.dot_general(a, b, (dims, ((), ())), preferred_element_type=F32)


NT = ((1,), (1,))


def hot(a, b):
    return (a == b).astype(BF)


def call(kernel, outs, *args, smem=0, rest=0):
    first = [pl.BlockSpec(memory_space=pltpu.SMEM)] * smem
    last = [pl.BlockSpec(memory_space=pl.ANY)] * rest
    return pl.pallas_call(
        kernel,
        out_shape=[jax.ShapeDtypeStruct(s, d) for s, d in outs],
        in_specs=first + [VM] * (len(args) - smem - rest) + last,
        out_specs=[VM] * len(outs),
    )(*args)


def quotient(n, by, top):
    shift = 0
    while (1 << shift) < by * top:
        shift += 1
    factor = -(-(1 << shift) // by)
    assert factor * top < 2**31
    return lax.shift_right_logical(n * factor, jnp.int32(shift))


def ring_rows(r, z, c, sizes):
    nz, piece, ls, cap, bl, slots = sizes
    half = nz * piece
    h = (r >= half).astype(jnp.int32)
    inner = r - half * h
    j = quotient(inner, piece, half)
    turn = (1 - 2 * c) * (1 - 2 * h) * j
    place = piece * (2 * ((z + turn) & (nz - 1)) + jnp.abs(c - h)) + inner - piece * j
    block = quotient(place, ls, 2 * half)
    within = place - ls * block
    routed = place < slots
    expert = jnp.where(routed, quotient(within, cap, ls), ls // cap)
    src = jnp.where(routed, block * bl + within, slots // ls * bl + place - slots)
    return src, expert, jnp.where(routed, block, -1), within


def along(n, dim):
    return lax.broadcasted_iota(jnp.int32, (n, 1) if dim == 0 else (1, n), dim)


def one_hot(a, b):
    return jnp.where(a == b, 1.0, 0.0).astype(BF)


def columns(lines):
    lines = lines.astype(F32)
    return jnp.concatenate([lines, jnp.zeros((8 - lines.shape[0], lines.shape[1]), F32)], 0).T


def routing(routes, le, cap, experts):
    top, rows = routes.shape
    routes = columns(routes).astype(jnp.int32)
    lanes = lax.broadcasted_iota(jnp.int32, (rows, experts), 1)
    chosen = [routes[:, k : k + 1] for k in range(top)]
    on = [jnp.where(f == lanes, 1.0, 0.0) for f in chosen]
    shape = (rows, rows)
    tri = jnp.where(lax.broadcasted_iota(jnp.int32, shape, 0) > lax.broadcasted_iota(jnp.int32, shape, 1), 1.0, 0.0)
    before = mm(tri.astype(BF), sum(on).astype(BF))
    out = []
    for f, o in zip(chosen, on):
        dest = quotient(f, le, experts)
        pos = jnp.sum(o * before, axis=1, keepdims=True).astype(jnp.int32)
        out.append((dest, (f - le * dest) * cap + pos))
    return out


def dispatch(geo, tokens, cotangent, routes, weights, sent, both):
    le, cap, experts, bl = geo
    rows, width = tokens.shape
    n = sent.shape[0]
    xg = jnp.concatenate([tokens[...], cotangent[...]], 1)
    both[...] = xg
    where = routing(routes[...], le, cap, experts)
    cols = lax.broadcasted_iota(jnp.int32, (rows, n), 1)
    lanes = lax.broadcasted_iota(jnp.int32, (rows, 2 * width), 1)
    w = columns(weights[...])
    left, right = [jnp.zeros((rows, n), F32)], [xg]
    for k, (dest, within) in enumerate(where):
        left[0] = left[0] + jnp.where(dest * bl + within == cols, 1.0, 0.0)
        left.append(jnp.where(dest * bl + le * cap == cols, w[:, k : k + 1], 0.0))
        right.append(one_hot(within, lanes))
    left = jnp.concatenate([a.T.astype(BF) for a in left], 1)
    sent[...] = mm(left, jnp.concatenate(right, 0)).astype(BF)


def collect(geo, home, shared, routes, after, token_grad, gate_grad):
    le, cap, experts, bl = geo
    n_ep = home.shape[0]
    rows, width = shared.shape
    n = n_ep * bl
    first = home.shape[1] - bl
    where = routing(routes[...], le, cap, experts)
    cols = lax.broadcasted_iota(jnp.int32, (rows, n), 1)
    lanes = lax.broadcasted_iota(jnp.int32, (rows, width), 1)
    back = home[:, first:, :].astype(F32).reshape(n, width).astype(BF)
    pick, picked = jnp.zeros((rows, n), F32), []
    for dest, within in where:
        pick = pick + jnp.where(dest * bl + within == cols, 1.0, 0.0)
        line = mm(one_hot(dest * bl + le * cap, cols), back)
        picked.append(jnp.sum(jnp.where(within == lanes, line, 0.0), axis=1, keepdims=True))
    picked.append(jnp.zeros((rows, 8 - len(picked)), F32))
    gate_grad[...] = jnp.concatenate(picked, 1).T[: gate_grad.shape[0]]
    token_grad[...] = (mm(pick.astype(BF), back) + shared[...]).astype(BF)


def gather_norms(home, quarter, shared, lines):
    _, cols, width = shared.shape
    hidden_rows = 3 * cols
    acc = home[0, :hidden_rows, :].astype(F32)
    for e in range(1, home.shape[0]):
        acc = acc + home[e, :hidden_rows, :].astype(F32)
    turned = acc.T
    for t in range(3):
        shared[t] = acc[t * cols : (t + 1) * cols]
    row = jnp.sum(turned * turned, axis=0, keepdims=True)
    fill = lines.shape[1] * width - quarter.shape[0] * width - hidden_rows
    row = jnp.concatenate([row, jnp.zeros((1, fill), F32)], 1)
    parts = [quarter[...]] + [row[:, a : a + width] for a in range(0, row.shape[1], width)]
    lines[...] = jnp.broadcast_to(jnp.concatenate(parts, 0).astype(BF)[None], lines.shape)


def finish_norms(scale, lines, e_norm, s_norm):
    n, block, width = lines.shape
    _, le, hidden = e_norm.shape
    cols = s_norm.shape[1]
    q = 3 * le * hidden // (4 * width)
    rows = []
    for c in range(2):
        for b in range(2):
            acc = lines[2 * b + c].astype(F32)
            for d in range(4 + 2 * b + c, n, 4):
                acc = acc + lines[d].astype(F32)
            rows.append(acc)
    whole = rows[0] + rows[1] + rows[2] + rows[3]
    rows = [r[i : i + 1] * scale for r in rows for i in range(q)]
    per = hidden // width
    for t in range(3):
        for e in range(le):
            at = (t * le + e) * per
            e_norm[t, e : e + 1, :] = jnp.concatenate(rows[at : at + per], 1)
    line = jnp.concatenate([whole[i : i + 1] for i in range(q, block)], 1) * scale
    for t in range(3):
        s_norm[t : t + 1, :] = line[:, t * cols : (t + 1) * cols]


def project(sizes, pos, got, both, eg, eu, ed, sg, su, sd, own_r, own_l, out_r, out_l, xt_ref, gt_ref, xs_ref, gs_ref):
    le, width, hidden = eg.shape
    nb, rows = got.shape[0], both.shape[0]
    nr, nl = own_r.shape[0], own_l.shape[0]
    half = nr + nl
    z, c = pos[0], pos[1]
    src, kd, _, _ = ring_rows(along(2 * half, 0), z, c, sizes)
    cols = lax.broadcasted_iota(jnp.int32, (2 * half, nb), 1)
    mine = mm(one_hot(src, cols), got[...])
    mine = mine + mm(one_hot(src - nb, lax.broadcasted_iota(jnp.int32, (2 * half, rows), 1)), both[...])
    part = [jnp.where(kd == e, mine, 0.0).astype(BF) for e in range(le + 1)]
    x = jnp.concatenate([p[:, :width] for p in part[:le]], 1)
    g = jnp.concatenate([p[:, width:] for p in part[:le]], 1)
    todo = ((x, part[le][:, :width], eg, sg), (x, part[le][:, :width], eu, su), (g, part[le][:, width:], ed, sd))
    for t, (xe, xs, we, ws) in enumerate(todo):
        cut = slice(t * hidden, (t + 1) * hidden)
        p = mm(xe, we[...].reshape(le * width, hidden)) + mm(xs, ws[...])
        own_r[:, cut] = p[:nr]
        own_l[:, cut] = p[nr:half]
        out_r[:, cut] = p[half : half + nr].astype(BF)
        out_l[:, cut] = p[half + nr :].astype(BF)
    _, kr, _, _ = ring_rows(along(2 * half, 1), z, c, sizes)
    mine_t = mine.T
    for e in range(le + 1):
        both_t = jnp.where(kr == e, mine_t, 0.0).astype(BF)
        to_x, to_g, at = (xt_ref, gt_ref, e * width) if e < le else (xs_ref, gs_ref, 0)
        to_x[at : at + width, :] = both_t[:width]
        to_g[at : at + width, :] = both_t[width:]


def over_rows(lhs, parts, cut):
    at, out = 0, None
    for p in parts:
        n = p.shape[0]
        r = mm(lhs[:, at : at + n], p[:, cut])
        out = r if out is None else out + r
        at += n
    return out


def expert_grads(kept, other, xt, gt, after, stack, sq):
    _, le, width, hidden = stack.shape
    for t, lhs in enumerate((xt, xt, gt)):
        r = over_rows(lhs, (kept, other), slice(t * hidden, (t + 1) * hidden)).reshape(le, width, hidden)
        stack[t] = r.astype(BF)
        total = jnp.sum(r * r, axis=1, keepdims=True)
        per = hidden // width
        for e in range(le):
            for q in range(per):
                at = (t * le + e) * per + q
                sq[at : at + 1, :] = total[e, :, q * width : (q + 1) * width]


def row_grads(sizes, pos, kept, other, eg, eu, sg, su, xs, gs, out, shared):
    le, width, hidden = eg.shape
    ls, bl = sizes[2], sizes[4]
    n_ep, rows = out.shape[0], shared.shape[0]
    nb = n_ep * bl
    cols = hidden // n_ep
    for t, lhs in enumerate((xs, xs, gs)):
        r = over_rows(lhs, (kept, other), slice(t * hidden, (t + 1) * hidden))
        out[:, t * cols : (t + 1) * cols, :] = r.T.astype(BF).reshape(n_ep, cols, width)
    total = 2 * sizes[0] * sizes[1]
    z, c = pos[0], pos[1]
    _, kd, _, within = ring_rows(along(total, 0), z, c, sizes)
    slots, wg, at = [], [], 0
    for src in (kept, other):
        n = src.shape[0]
        gg, gu = src[:, :hidden], src[:, hidden : 2 * hidden]
        se = mm(gg, eg[...].reshape(le * width, hidden), NT) + mm(gu, eu[...].reshape(le * width, hidden), NT)
        ss = mm(gg, sg[...], NT) + mm(gu, su[...], NT)
        k = kd[at : at + n]
        s = jnp.where(k == le, ss, 0.0)
        for e in range(le):
            s = s + jnp.where(k == e, se[:, e * width : (e + 1) * width], 0.0)
        slots.append(s)
        lanes = lax.broadcasted_iota(jnp.int32, (n, width), 1)
        wg.append(jnp.where(within[at : at + n] == lanes, src[:, 3 * hidden :].astype(F32), 0.0))
        at += n
    slot = jnp.concatenate(slots, 0)
    hi = slot.astype(BF)
    rest = slot - hi.astype(F32)
    mid = rest.astype(BF)
    low = (rest - mid.astype(F32)).astype(BF)
    src_r, _, block, _ = ring_rows(along(total, 1), z, c, sizes)
    lines = lax.broadcasted_iota(jnp.int32, (nb, total), 0)
    to_slot = one_hot(lines, src_r)
    to_tail = one_hot(lines, jnp.where(block >= 0, block * bl + ls, -1))
    back = mm(to_slot, hi) + mm(to_tail, jnp.concatenate(wg, 0).astype(BF))
    out[:, 3 * cols :, :] = back.reshape(n_ep, bl, width).astype(BF)
    ps = one_hot(lax.broadcasted_iota(jnp.int32, (rows, total), 0) + nb, src_r)
    shared[...] = mm(ps, hi) + mm(ps, mid) + mm(ps, low)


def row_backward(summed, weights):
    hidden = summed.shape[1] // 3
    pre_gate = summed[:, :hidden]
    pre_up = summed[:, hidden : 2 * hidden]
    back_act = summed[:, 2 * hidden :]
    sigmoid_gate = jax.nn.sigmoid(pre_gate)
    silu_gate = pre_gate * sigmoid_gate
    activation = silu_gate * pre_up
    act_grad = weights * back_act
    grad_up = (act_grad * silu_gate).astype(BF)
    grad_gate = (act_grad * pre_up * sigmoid_gate * (1.0 + pre_gate * (1.0 - sigmoid_gate))).astype(BF)
    scaled_act = (weights * activation).astype(BF)
    weight_grad = jnp.sum(activation * back_act, axis=1, keepdims=True).astype(BF)
    return grad_gate, grad_up, scaled_act, weight_grad


def body(tokens, cotangent, routes, gate_weights, e_gate, e_up, e_down, s_gate, s_up, s_down):
    n_ep, n_tp = lax.axis_size("ep"), lax.axis_size("tp")
    nz = n_tp // 2
    rows, width = tokens.shape
    top = routes.shape[1]
    le, _, hidden = e_gate.shape
    experts = le * n_ep
    cap = 3 * rows * top // (2 * experts)
    ls = le * cap
    bl = (ls + 8) // 8 * 8
    slots = n_ep * ls
    total = slots + rows
    piece = total // n_tp
    tp = lax.axis_index("tp")
    z, c = tp // 2, tp % 2
    fwd = [(i, (i + 2 - 4 * (i % 2)) % n_tp) for i in range(n_tp)]
    bwd = [(i, (i - 2 + 4 * (i % 2)) % n_tp) for i in range(n_tp)]
    swap = [(i, i ^ 1) for i in range(n_tp)]

    geo = (le, cap, experts, bl)
    lanes = jnp.arange(2 * width, dtype=jnp.int32)
    groups = jnp.arange(n_ep, dtype=jnp.int32)
    sent, both = call(
        functools.partial(dispatch, geo),
        [((n_ep * bl, 2 * width), BF), ((rows, 2 * width), BF)],
        tokens, cotangent, routes.T, gate_weights.T,
    )
    got = lax.all_to_all(sent.reshape(n_ep, bl, 2 * width), "ep", 0, 0, tiled=True)

    sizes = (nz, piece, ls, cap, bl, slots)
    pos = jnp.stack([z, c]).astype(jnp.int32)
    hops, back_hops = nz // 2, nz - nz // 2 - 1
    nr, nl = (hops + 1) * piece, back_hops * piece
    width3 = 3 * hidden
    own_r, own_l, out_r, out_l, xt, gt, xs, gs = call(
        functools.partial(project, sizes),
        [((nr, width3), F32), ((nl, width3), F32), ((nr, width3), BF), ((nl, width3), BF)]
        + [((le * width, total), BF)] * 2
        + [((width, total), BF)] * 2,
        pos, got.reshape(n_ep * bl, 2 * width), both, e_gate, e_up, e_down, s_gate, s_up, s_down, smem=1,
    )
    oth_r = lax.ppermute(out_r, "tp", swap)
    oth_l = lax.ppermute(out_l, "tp", swap)

    def at_r(j):
        rows_j = slice(j * piece, (j + 1) * piece)
        return own_r[rows_j] + oth_r[rows_j].astype(F32)

    def at_l(j):
        rows_j = slice((back_hops - j) * piece, (back_hops - j + 1) * piece)
        return own_l[rows_j] + oth_l[rows_j].astype(F32)

    right, left = at_r(hops).astype(BF), at_l(back_hops).astype(BF)
    for t in range(hops):
        right = lax.ppermute(right, "tp", fwd)
        if t < hops - 1:
            right = right.astype(F32) + at_r(hops - 1 - t)
            right = right if t == hops - 2 else right.astype(BF)
        if t < back_hops:
            left = lax.ppermute(left, "tp", bwd)
        if t < back_hops - 1:
            left = left.astype(F32) + at_l(back_hops - 1 - t)
            left = left if t == back_hops - 2 else left.astype(BF)
    summed = right.astype(F32) + left.astype(F32) + at_r(0)

    q = tp * piece + jnp.arange(piece, dtype=jnp.int32)
    w_rows = mm(hot((q // ls)[:, None], groups[None, :]), got[:, ls, :])
    own_w = jnp.sum(jnp.where((q % ls)[:, None] == lanes[None, :], w_rows, 0.0), axis=1)
    own_w = jnp.where(q < slots, own_w, 1.0)[:, None]
    gg, gu, sa, wg = row_backward(summed, own_w)
    block = jnp.concatenate([gg, gu, sa, jnp.broadcast_to(wg, (piece, 128))], 1)

    ring = [None] * nz
    ring[0] = right = left = block
    for t in range(1, hops + 1):
        right = lax.ppermute(right, "tp", fwd)
        ring[-t % nz] = right
        if t <= back_hops:
            left = lax.ppermute(left, "tp", bwd)
            ring[t] = left
    kept = jnp.concatenate(ring, 0)
    grads = (kept, lax.ppermute(kept, "tp", swap))

    cols = hidden // n_ep
    out, shared_part = call(
        functools.partial(row_grads, sizes),
        [((n_ep, 3 * cols + bl, width), BF), ((rows, width), F32)],
        pos, *grads, e_gate, e_up, s_gate, s_up, xs, gs, smem=1,
    )
    home = lax.all_to_all(out, "ep", 0, 0, tiled=True)
    stack, e_sq = call(
        expert_grads, [((3, le, width, hidden), BF), ((3 * le * hidden // width, width), F32)], *grads, xt, gt, out, rest=1
    )
    e_sq = e_sq.reshape(2, -1, width)
    other_sq = lax.ppermute(jnp.where(c == 0, e_sq[1], e_sq[0]), "tp", swap)
    e_sq = (jnp.where(c == 0, e_sq[0], e_sq[1]) + other_sq).reshape(2, -1, width)
    other_sq = lax.ppermute(jnp.where(z % 2 == 0, e_sq[1], e_sq[0]), "tp", [(i, i ^ 2) for i in range(n_tp)])
    e_sq = jnp.where(z % 2 == 0, e_sq[0], e_sq[1]) + other_sq
    n_lines = (e_sq.shape[0] + -(-3 * cols // width) + 15) // 16 * 16
    shared, lines = call(
        gather_norms, [((3, cols, width), F32), ((n_tp, n_lines, width), BF)], home, e_sq
    )
    got_lines = lax.all_to_all(lines, "tp", 0, 0, tiled=True)
    token_grad, gate_grad = call(
        functools.partial(collect, geo),
        [((rows, width), BF), ((top, rows), F32)],
        home, shared_part, routes.T, lines, rest=1,
    )
    e_norm, s_norm = call(
        functools.partial(finish_norms, 1.0 / (width * n_tp)),
        [((3, le, hidden), F32), ((3, cols), F32)],
        got_lines,
    )
    return token_grad, gate_grad.astype(BF).T, stack, jnp.swapaxes(shared, 1, 2), e_norm, s_norm


def solution(mesh):
    return jax.shard_map(
        body,
        mesh=mesh,
        in_specs=(
            P("ep", "tp"),
            P("ep", "tp"),
            P("ep", None),
            P("ep", None),
            P("ep", "tp", None),
            P("ep", "tp", None),
            P("ep", "tp", None),
            P("tp", None),
            P("tp", None),
            P("tp", None),
        ),
        out_specs=(
            P("ep", "tp"),
            P("ep", None),
            P(None, "ep", "tp", None),
            P(None, "tp", "ep"),
            P(None, "ep", None),
            P(None, "ep"),
        ),
        check_vma=False,
    )
```

```python
import functools

import jax
import jax.numpy as jnp
from jax import lax
from jax.experimental import pallas as pl
from jax.experimental.pallas import tpu as pltpu
from jax.sharding import PartitionSpec as P


BF = jnp.bfloat16
F32 = jnp.float32
VM = pl.BlockSpec(memory_space=pltpu.VMEM)


def mm(a, b, dims=((1,), (0,))):
    return lax.dot_general(a, b, (dims, ((), ())), preferred_element_type=F32)


NT = ((1,), (1,))


def hot(a, b):
    return (a == b).astype(BF)


def call(kernel, outs, *args, smem=0, rest=0):
    first = [pl.BlockSpec(memory_space=pltpu.SMEM)] * smem
    last = [pl.BlockSpec(memory_space=pl.ANY)] * rest
    return pl.pallas_call(
        kernel,
        out_shape=[jax.ShapeDtypeStruct(s, d) for s, d in outs],
        in_specs=first + [VM] * (len(args) - smem - rest) + last,
        out_specs=[VM] * len(outs),
    )(*args)


def quotient(n, by, top):
    shift = 0
    while (1 << shift) < by * top:
        shift += 1
    factor = -(-(1 << shift) // by)
    assert factor * top < 2**31
    return lax.shift_right_logical(n * factor, jnp.int32(shift))


def ring_rows(r, z, c, sizes):
    nz, piece, ls, cap, bl, slots = sizes
    sec = nz // 2 * piece
    half = 2 * sec
    h = (r >= half).astype(jnp.int32)
    inner = r - half * h
    q = (inner >= sec).astype(jnp.int32)
    inner = inner - sec * q
    m = quotient(inner, piece, sec)
    core = jnp.abs(c - h)
    zeta = (z + core) & (nz - 1)
    zeta = zeta + q * (1 - 2 * (zeta & 1)) + 2 * (1 - 2 * core) * m
    place = piece * (2 * ((zeta - core) & (nz - 1)) + core) + inner - piece * m
    block = quotient(place, ls, 2 * half)
    within = place - ls * block
    routed = place < slots
    expert = jnp.where(routed, quotient(within, cap, ls), ls // cap)
    src = jnp.where(routed, block * bl + within, slots // ls * bl + place - slots)
    return src, expert, jnp.where(routed, block, -1), within


def along(n, dim):
    return lax.broadcasted_iota(jnp.int32, (n, 1) if dim == 0 else (1, n), dim)


def one_hot(a, b):
    return jnp.where(a == b, 1.0, 0.0).astype(BF)


def columns(lines):
    lines = lines.astype(F32)
    return jnp.concatenate([lines, jnp.zeros((8 - lines.shape[0], lines.shape[1]), F32)], 0).T


def routing(routes, le, cap, experts):
    top, rows = routes.shape
    routes = columns(routes).astype(jnp.int32)
    lanes = lax.broadcasted_iota(jnp.int32, (rows, experts), 1)
    chosen = [routes[:, k : k + 1] for k in range(top)]
    on = [jnp.where(f == lanes, 1.0, 0.0) for f in chosen]
    shape = (rows, rows)
    tri = jnp.where(lax.broadcasted_iota(jnp.int32, shape, 0) > lax.broadcasted_iota(jnp.int32, shape, 1), 1.0, 0.0)
    before = mm(tri.astype(BF), sum(on).astype(BF))
    out = []
    for f, o in zip(chosen, on):
        dest = quotient(f, le, experts)
        pos = jnp.sum(o * before, axis=1, keepdims=True).astype(jnp.int32)
        out.append((dest, (f - le * dest) * cap + pos))
    return out


def dispatch(geo, tokens, cotangent, routes, weights, sent, both):
    le, cap, experts, bl = geo
    rows, width = tokens.shape
    n = sent.shape[0]
    xg = jnp.concatenate([tokens[...], cotangent[...]], 1)
    both[...] = xg
    where = routing(routes[...], le, cap, experts)
    cols = lax.broadcasted_iota(jnp.int32, (rows, n), 1)
    lanes = lax.broadcasted_iota(jnp.int32, (rows, 2 * width), 1)
    w = columns(weights[...])
    left, right = [jnp.zeros((rows, n), F32)], [xg]
    for k, (dest, within) in enumerate(where):
        left[0] = left[0] + jnp.where(dest * bl + within == cols, 1.0, 0.0)
        left.append(jnp.where(dest * bl + le * cap == cols, w[:, k : k + 1], 0.0))
        right.append(one_hot(within, lanes))
    left = jnp.concatenate([a.T.astype(BF) for a in left], 1)
    sent[...] = mm(left, jnp.concatenate(right, 0)).astype(BF)


def collect(geo, home, shared, routes, after, token_grad, gate_grad):
    le, cap, experts, bl = geo
    n_ep = home.shape[0]
    rows, width = shared.shape
    n = n_ep * bl
    first = home.shape[1] - bl
    where = routing(routes[...], le, cap, experts)
    cols = lax.broadcasted_iota(jnp.int32, (rows, n), 1)
    lanes = lax.broadcasted_iota(jnp.int32, (rows, width), 1)
    back = home[:, first:, :].astype(F32).reshape(n, width).astype(BF)
    pick, picked = jnp.zeros((rows, n), F32), []
    for dest, within in where:
        pick = pick + jnp.where(dest * bl + within == cols, 1.0, 0.0)
        line = mm(one_hot(dest * bl + le * cap, cols), back)
        picked.append(jnp.sum(jnp.where(within == lanes, line, 0.0), axis=1, keepdims=True))
    picked.append(jnp.zeros((rows, 8 - len(picked)), F32))
    gate_grad[...] = jnp.concatenate(picked, 1).T[: gate_grad.shape[0]]
    token_grad[...] = (mm(pick.astype(BF), back) + shared[...]).astype(BF)


def gather_norms(home, quarter, shared, lines):
    _, cols, width = shared.shape
    hidden_rows = 3 * cols
    acc = home[0, :hidden_rows, :].astype(F32)
    for e in range(1, home.shape[0]):
        acc = acc + home[e, :hidden_rows, :].astype(F32)
    turned = acc.T
    for t in range(3):
        shared[t] = acc[t * cols : (t + 1) * cols]
    row = jnp.sum(turned * turned, axis=0, keepdims=True)
    fill = lines.shape[1] * width - quarter.shape[0] * width - hidden_rows
    row = jnp.concatenate([row, jnp.zeros((1, fill), F32)], 1)
    parts = [quarter[...]] + [row[:, a : a + width] for a in range(0, row.shape[1], width)]
    lines[...] = jnp.broadcast_to(jnp.concatenate(parts, 0).astype(BF)[None], lines.shape)


def finish_norms(scale, lines, e_norm, s_norm):
    n, block, width = lines.shape
    _, le, hidden = e_norm.shape
    cols = s_norm.shape[1]
    q = 3 * le * hidden // (4 * width)
    rows = []
    for c in range(2):
        for b in range(2):
            acc = lines[2 * b + c].astype(F32)
            for d in range(4 + 2 * b + c, n, 4):
                acc = acc + lines[d].astype(F32)
            rows.append(acc)
    whole = rows[0] + rows[1] + rows[2] + rows[3]
    rows = [r[i : i + 1] * scale for r in rows for i in range(q)]
    per = hidden // width
    for t in range(3):
        for e in range(le):
            at = (t * le + e) * per
            e_norm[t, e : e + 1, :] = jnp.concatenate(rows[at : at + per], 1)
    line = jnp.concatenate([whole[i : i + 1] for i in range(q, block)], 1) * scale
    for t in range(3):
        s_norm[t : t + 1, :] = line[:, t * cols : (t + 1) * cols]


def project(sizes, pos, got, both, eg, eu, ed, sg, su, sd, own_r, own_l, out_r, out_l, xt_ref, gt_ref, xs_ref, gs_ref):
    le, width, hidden = eg.shape
    nb, rows = got.shape[0], both.shape[0]
    nr, nl = own_r.shape[0], own_l.shape[0]
    half = nr + nl
    z, c = pos[0], pos[1]
    src, kd, _, _ = ring_rows(along(2 * half, 0), z, c, sizes)
    cols = lax.broadcasted_iota(jnp.int32, (2 * half, nb), 1)
    mine = mm(one_hot(src, cols), got[...])
    mine = mine + mm(one_hot(src - nb, lax.broadcasted_iota(jnp.int32, (2 * half, rows), 1)), both[...])
    part = [jnp.where(kd == e, mine, 0.0).astype(BF) for e in range(le + 1)]
    x = jnp.concatenate([p[:, :width] for p in part[:le]], 1)
    g = jnp.concatenate([p[:, width:] for p in part[:le]], 1)
    todo = ((x, part[le][:, :width], eg, sg), (x, part[le][:, :width], eu, su), (g, part[le][:, width:], ed, sd))
    for t, (xe, xs, we, ws) in enumerate(todo):
        cut = slice(t * hidden, (t + 1) * hidden)
        p = mm(xe, we[...].reshape(le * width, hidden)) + mm(xs, ws[...])
        own_r[:, cut] = p[:nr]
        own_l[:, cut] = p[nr:half]
        out_r[:, cut] = p[half : half + nr].astype(BF)
        out_l[:, cut] = p[half + nr :].astype(BF)
    _, kr, _, _ = ring_rows(along(2 * half, 1), z, c, sizes)
    mine_t = mine.T
    for e in range(le + 1):
        both_t = jnp.where(kr == e, mine_t, 0.0).astype(BF)
        to_x, to_g, at = (xt_ref, gt_ref, e * width) if e < le else (xs_ref, gs_ref, 0)
        to_x[at : at + width, :] = both_t[:width]
        to_g[at : at + width, :] = both_t[width:]


def over_rows(lhs, parts, cut):
    at, out = 0, None
    for p in parts:
        n = p.shape[0]
        r = mm(lhs[:, at : at + n], p[:, cut])
        out = r if out is None else out + r
        at += n
    return out


def expert_grads(kept, other, xt, gt, after, stack, sq):
    _, le, width, hidden = stack.shape
    for t, lhs in enumerate((xt, xt, gt)):
        r = over_rows(lhs, (kept, other), slice(t * hidden, (t + 1) * hidden)).reshape(le, width, hidden)
        stack[t] = r.astype(BF)
        total = jnp.sum(r * r, axis=1, keepdims=True)
        per = hidden // width
        for e in range(le):
            for q in range(per):
                at = (t * le + e) * per + q
                sq[at : at + 1, :] = total[e, :, q * width : (q + 1) * width]


def row_grads(sizes, pos, kept, other, eg, eu, sg, su, xs, gs, out, shared):
    le, width, hidden = eg.shape
    ls, bl = sizes[2], sizes[4]
    n_ep, rows = out.shape[0], shared.shape[0]
    nb = n_ep * bl
    cols = hidden // n_ep
    for t, lhs in enumerate((xs, xs, gs)):
        r = over_rows(lhs, (kept, other), slice(t * hidden, (t + 1) * hidden))
        out[:, t * cols : (t + 1) * cols, :] = r.T.astype(BF).reshape(n_ep, cols, width)
    total = 2 * sizes[0] * sizes[1]
    z, c = pos[0], pos[1]
    _, kd, _, within = ring_rows(along(total, 0), z, c, sizes)
    slots, wg, at = [], [], 0
    for src in (kept, other):
        n = src.shape[0]
        gg, gu = src[:, :hidden], src[:, hidden : 2 * hidden]
        se = mm(gg, eg[...].reshape(le * width, hidden), NT) + mm(gu, eu[...].reshape(le * width, hidden), NT)
        ss = mm(gg, sg[...], NT) + mm(gu, su[...], NT)
        k = kd[at : at + n]
        s = jnp.where(k == le, ss, 0.0)
        for e in range(le):
            s = s + jnp.where(k == e, se[:, e * width : (e + 1) * width], 0.0)
        slots.append(s)
        lanes = lax.broadcasted_iota(jnp.int32, (n, width), 1)
        wg.append(jnp.where(within[at : at + n] == lanes, src[:, 3 * hidden :].astype(F32), 0.0))
        at += n
    slot = jnp.concatenate(slots, 0)
    hi = slot.astype(BF)
    rest = slot - hi.astype(F32)
    mid = rest.astype(BF)
    low = (rest - mid.astype(F32)).astype(BF)
    src_r, _, block, _ = ring_rows(along(total, 1), z, c, sizes)
    lines = lax.broadcasted_iota(jnp.int32, (nb, total), 0)
    to_slot = one_hot(lines, src_r)
    to_tail = one_hot(lines, jnp.where(block >= 0, block * bl + ls, -1))
    back = mm(to_slot, hi) + mm(to_tail, jnp.concatenate(wg, 0).astype(BF))
    out[:, 3 * cols :, :] = back.reshape(n_ep, bl, width).astype(BF)
    ps = one_hot(lax.broadcasted_iota(jnp.int32, (rows, total), 0) + nb, src_r)
    shared[...] = mm(ps, hi) + mm(ps, mid) + mm(ps, low)


def row_backward(summed, weights):
    hidden = summed.shape[1] // 3
    pre_gate = summed[:, :hidden]
    pre_up = summed[:, hidden : 2 * hidden]
    back_act = summed[:, 2 * hidden :]
    sigmoid_gate = jax.nn.sigmoid(pre_gate)
    silu_gate = pre_gate * sigmoid_gate
    activation = silu_gate * pre_up
    act_grad = weights * back_act
    grad_up = (act_grad * silu_gate).astype(BF)
    grad_gate = (act_grad * pre_up * sigmoid_gate * (1.0 + pre_gate * (1.0 - sigmoid_gate))).astype(BF)
    scaled_act = (weights * activation).astype(BF)
    weight_grad = jnp.sum(activation * back_act, axis=1, keepdims=True).astype(BF)
    return grad_gate, grad_up, scaled_act, weight_grad


def body(tokens, cotangent, routes, gate_weights, e_gate, e_up, e_down, s_gate, s_up, s_down):
    n_ep, n_tp = lax.axis_size("ep"), lax.axis_size("tp")
    nz = n_tp // 2
    rows, width = tokens.shape
    top = routes.shape[1]
    le, _, hidden = e_gate.shape
    experts = le * n_ep
    cap = 3 * rows * top // (2 * experts)
    ls = le * cap
    bl = (ls + 8) // 8 * 8
    slots = n_ep * ls
    total = slots + rows
    piece = total // n_tp
    tp = lax.axis_index("tp")
    z, c = tp // 2, tp % 2
    fwd = [(i, (i + 4 - 8 * (i % 2)) % n_tp) for i in range(n_tp)]
    bwd = [(b, a) for a, b in fwd]
    pair = [(i, (2 * ((i // 2 + i % 2) % nz ^ 1) - i % 2) % n_tp) for i in range(n_tp)]
    swap = [(i, i ^ 1) for i in range(n_tp)]

    geo = (le, cap, experts, bl)
    lanes = jnp.arange(2 * width, dtype=jnp.int32)
    groups = jnp.arange(n_ep, dtype=jnp.int32)
    sent, both = call(
        functools.partial(dispatch, geo),
        [((n_ep * bl, 2 * width), BF), ((rows, 2 * width), BF)],
        tokens, cotangent, routes.T, gate_weights.T,
    )
    got = lax.all_to_all(sent.reshape(n_ep, bl, 2 * width), "ep", 0, 0, tiled=True)

    sizes = (nz, piece, ls, cap, bl, slots)
    pos = jnp.stack([z, c]).astype(jnp.int32)
    members = nz // 2
    hops, back_hops = members // 2, members - members // 2 - 1
    sec = members * piece
    width3 = 3 * hidden
    own_k, own_s, out_k, out_s, xt, gt, xs, gs = call(
        functools.partial(project, sizes),
        [((sec, width3), F32)] * 2 + [((sec, width3), BF)] * 2 + [((le * width, total), BF)] * 2 + [((width, total), BF)] * 2,
        pos, got.reshape(n_ep * bl, 2 * width), both, e_gate, e_up, e_down, s_gate, s_up, s_down, smem=1,
    )
    oth_s = lax.ppermute(out_s, "tp", swap)
    oth_k = lax.ppermute(out_k, "tp", swap)
    cut = hops * piece
    to_hi = (own_s[cut:] + oth_s[cut:].astype(F32)).astype(BF)
    to_lo = (own_s[:cut] + oth_s[:cut].astype(F32)).astype(BF)
    par_hi = lax.ppermute(to_hi, "tp", pair)
    par_lo = lax.ppermute(to_lo, "tp", pair)

    on_left = lax.optimization_barrier((own_k[cut + piece :], oth_k[cut + piece :], par_hi[piece:]))

    def at(m):
        if m > hops:
            rows_m = slice((m - hops - 1) * piece, (m - hops) * piece)
            return sum(a[rows_m].astype(F32) for a in on_left)
        rows_m = slice(m * piece, (m + 1) * piece)
        par = par_lo[rows_m] if m < hops else par_hi[m * piece - cut : (m + 1) * piece - cut]
        return own_k[rows_m] + oth_k[rows_m].astype(F32) + par.astype(F32)

    right, left = at(hops).astype(BF), at(hops + 1).astype(BF)
    for t in range(hops):
        right = lax.ppermute(right, "tp", fwd)
        if t < hops - 1:
            right = (right.astype(F32) + at(hops - 1 - t)).astype(BF)
        if t < back_hops:
            left = lax.ppermute(left, "tp", bwd)
        if t < back_hops - 1:
            left = (left.astype(F32) + at(hops + 2 + t)).astype(BF)
    summed = right.astype(F32) + left.astype(F32) + at(0)

    q = tp * piece + jnp.arange(piece, dtype=jnp.int32)
    w_rows = mm(hot((q // ls)[:, None], groups[None, :]), got[:, ls, :])
    own_w = jnp.sum(jnp.where((q % ls)[:, None] == lanes[None, :], w_rows, 0.0), axis=1)
    own_w = jnp.where(q < slots, own_w, 1.0)[:, None]
    gg, gu, sa, wg = row_backward(summed, own_w)
    block = jnp.concatenate([gg, gu, sa, jnp.broadcast_to(wg, (piece, 128))], 1)

    ring = [None] * members
    ring[0] = right = left = block
    for t in range(1, hops + 1):
        right = lax.ppermute(right, "tp", fwd)
        ring[-t % members] = right
        if t <= back_hops:
            left = lax.ppermute(left, "tp", bwd)
            ring[t] = left
    lo = jnp.concatenate(ring[:hops], 0)
    hi = jnp.concatenate(ring[hops:], 0)
    lo_o = lax.ppermute(lo, "tp", pair)
    hi_o = lax.ppermute(hi, "tp", pair)
    kept = jnp.concatenate([lo, hi, lo_o, hi_o], 0)
    grads = (kept, lax.ppermute(kept, "tp", swap))

    cols = hidden // n_ep
    out, shared_part = call(
        functools.partial(row_grads, sizes),
        [((n_ep, 3 * cols + bl, width), BF), ((rows, width), F32)],
        pos, *grads, e_gate, e_up, s_gate, s_up, xs, gs, smem=1,
    )
    home = lax.all_to_all(out, "ep", 0, 0, tiled=True)
    stack, e_sq = call(
        expert_grads, [((3, le, width, hidden), BF), ((3 * le * hidden // width, width), F32)], *grads, xt, gt, out, rest=1
    )
    e_sq = e_sq.reshape(2, -1, width)
    other_sq = lax.ppermute(jnp.where(c == 0, e_sq[1], e_sq[0]), "tp", swap)
    e_sq = (jnp.where(c == 0, e_sq[0], e_sq[1]) + other_sq).reshape(2, -1, width)
    other_sq = lax.ppermute(jnp.where(z % 2 == 0, e_sq[1], e_sq[0]), "tp", [(i, i ^ 2) for i in range(n_tp)])
    e_sq = jnp.where(z % 2 == 0, e_sq[0], e_sq[1]) + other_sq
    n_lines = (e_sq.shape[0] + -(-3 * cols // width) + 15) // 16 * 16
    shared, lines = call(
        gather_norms, [((3, cols, width), F32), ((n_tp, n_lines, width), BF)], home, e_sq
    )
    got_lines = lax.all_to_all(lines, "tp", 0, 0, tiled=True)
    token_grad, gate_grad = call(
        functools.partial(collect, geo),
        [((rows, width), BF), ((top, rows), F32)],
        home, shared_part, routes.T, lines, rest=1,
    )
    e_norm, s_norm = call(
        functools.partial(finish_norms, 1.0 / (width * n_tp)),
        [((3, le, hidden), F32), ((3, cols), F32)],
        got_lines,
    )
    return token_grad, gate_grad.astype(BF).T, stack, jnp.swapaxes(shared, 1, 2), e_norm, s_norm


def solution(mesh):
    return jax.shard_map(
        body,
        mesh=mesh,
        in_specs=(
            P("ep", "tp"),
            P("ep", "tp"),
            P("ep", None),
            P("ep", None),
            P("ep", "tp", None),
            P("ep", "tp", None),
            P("ep", "tp", None),
            P("tp", None),
            P("tp", None),
            P("tp", None),
        ),
        out_specs=(
            P("ep", "tp"),
            P("ep", None),
            P(None, "ep", "tp", None),
            P(None, "tp", "ep"),
            P(None, "ep", None),
            P(None, "ep"),
        ),
        check_vma=False,
    )
```

```python
import functools

import jax
import jax.numpy as jnp
from jax import lax
from jax.experimental import pallas as pl
from jax.experimental.pallas import tpu as pltpu
from jax.sharding import PartitionSpec as P


BF = jnp.bfloat16
F32 = jnp.float32
VM = pl.BlockSpec(memory_space=pltpu.VMEM)


def mm(a, b, dims=((1,), (0,))):
    return lax.dot_general(a, b, (dims, ((), ())), preferred_element_type=F32)


NT = ((1,), (1,))


def hot(a, b):
    return (a == b).astype(BF)


def call(kernel, outs, *args, smem=0, rest=0, limit=None):
    first = [pl.BlockSpec(memory_space=pltpu.SMEM)] * smem
    last = [pl.BlockSpec(memory_space=pl.ANY)] * rest
    return pl.pallas_call(
        kernel,
        out_shape=[jax.ShapeDtypeStruct(s, d) for s, d in outs],
        in_specs=first + [VM] * (len(args) - smem - rest) + last,
        out_specs=[VM] * len(outs),
        compiler_params=pltpu.CompilerParams(vmem_limit_bytes=limit),
    )(*args)


def quotient(n, by, top):
    shift = 0
    while (1 << shift) < by * top:
        shift += 1
    factor = -(-(1 << shift) // by)
    assert factor * top < 2**31
    return lax.shift_right_logical(n * factor, jnp.int32(shift))


def ring_rows(r, z, c, sizes):
    nz, piece, ls, cap, bl, slots = sizes
    sec = nz // 2 * piece
    half = 2 * sec
    h = (r >= half).astype(jnp.int32)
    inner = r - half * h
    q = (inner >= sec).astype(jnp.int32)
    inner = inner - sec * q
    m = quotient(inner, piece, sec)
    core = jnp.abs(c - h)
    zeta = (z + core) & (nz - 1)
    zeta = zeta + q * (1 - 2 * (zeta & 1)) + 2 * (1 - 2 * core) * (m + nz // 4)
    place = piece * (2 * ((zeta - core) & (nz - 1)) + core) + inner - piece * m
    block = quotient(place, ls, 2 * half)
    within = place - ls * block
    routed = place < slots
    expert = jnp.where(routed, quotient(within, cap, ls), ls // cap)
    src = jnp.where(routed, block * bl + within, slots // ls * bl + place - slots)
    return src, expert, jnp.where(routed, block, -1), within


def along(n, dim):
    return lax.broadcasted_iota(jnp.int32, (n, 1) if dim == 0 else (1, n), dim)


def one_hot(a, b):
    return jnp.where(a == b, 1.0, 0.0).astype(BF)


def columns(lines):
    lines = lines.astype(F32)
    return jnp.concatenate([lines, jnp.zeros((8 - lines.shape[0], lines.shape[1]), F32)], 0).T


def routing(routes, le, cap, experts):
    top, rows = routes.shape
    routes = columns(routes).astype(jnp.int32)
    lanes = lax.broadcasted_iota(jnp.int32, (rows, experts), 1)
    chosen = [routes[:, k : k + 1] for k in range(top)]
    on = [jnp.where(f == lanes, 1.0, 0.0) for f in chosen]
    shape = (rows, rows)
    tri = jnp.where(lax.broadcasted_iota(jnp.int32, shape, 0) > lax.broadcasted_iota(jnp.int32, shape, 1), 1.0, 0.0)
    before = mm(tri.astype(BF), sum(on).astype(BF))
    out = []
    for f, o in zip(chosen, on):
        dest = quotient(f, le, experts)
        pos = jnp.sum(o * before, axis=1, keepdims=True).astype(jnp.int32)
        out.append((dest, (f - le * dest) * cap + pos))
    return out


def dispatch(geo, tokens, cotangent, routes, weights, sent, both):
    le, cap, experts, bl = geo
    rows, width = tokens.shape
    n = sent.shape[0]
    xg = jnp.concatenate([tokens[...], cotangent[...]], 1)
    both[...] = xg
    where = routing(routes[...], le, cap, experts)
    cols = lax.broadcasted_iota(jnp.int32, (rows, n), 1)
    lanes = lax.broadcasted_iota(jnp.int32, (rows, 2 * width), 1)
    w = columns(weights[...])
    left, right = [jnp.zeros((rows, n), F32)], [xg]
    for k, (dest, within) in enumerate(where):
        left[0] = left[0] + jnp.where(dest * bl + within == cols, 1.0, 0.0)
        left.append(jnp.where(dest * bl + le * cap == cols, w[:, k : k + 1], 0.0))
        right.append(one_hot(within, lanes))
    left = jnp.concatenate([a.T.astype(BF) for a in left], 1)
    sent[...] = mm(left, jnp.concatenate(right, 0)).astype(BF)


def collect(geo, home, shared, routes, after, token_grad, gate_grad):
    le, cap, experts, bl = geo
    n_ep = home.shape[0]
    rows, width = shared.shape
    n = n_ep * bl
    first = home.shape[1] - bl
    where = routing(routes[...], le, cap, experts)
    cols = lax.broadcasted_iota(jnp.int32, (rows, n), 1)
    lanes = lax.broadcasted_iota(jnp.int32, (rows, width), 1)
    back = home[:, first:, :].astype(F32).reshape(n, width).astype(BF)
    pick, picked = jnp.zeros((rows, n), F32), []
    for dest, within in where:
        pick = pick + jnp.where(dest * bl + within == cols, 1.0, 0.0)
        line = mm(one_hot(dest * bl + le * cap, cols), back)
        picked.append(jnp.sum(jnp.where(within == lanes, line, 0.0), axis=1, keepdims=True))
    picked.append(jnp.zeros((rows, 8 - len(picked)), F32))
    gate_grad[...] = jnp.concatenate(picked, 1).T[: gate_grad.shape[0]]
    token_grad[...] = (mm(pick.astype(BF), back) + shared[...]).astype(BF)


def gather_norms(home, quarter, shared, lines):
    _, cols, width = shared.shape
    hidden_rows = 3 * cols
    acc = home[0, :hidden_rows, :].astype(F32)
    for e in range(1, home.shape[0]):
        acc = acc + home[e, :hidden_rows, :].astype(F32)
    turned = acc.T
    for t in range(3):
        shared[t] = acc[t * cols : (t + 1) * cols]
    row = jnp.sum(turned * turned, axis=0, keepdims=True)
    fill = lines.shape[1] * width - quarter.shape[0] * width - hidden_rows
    row = jnp.concatenate([row, jnp.zeros((1, fill), F32)], 1)
    parts = [quarter[...]] + [row[:, a : a + width] for a in range(0, row.shape[1], width)]
    lines[...] = jnp.broadcast_to(jnp.concatenate(parts, 0).astype(BF)[None], lines.shape)


def finish_norms(scale, lines, e_norm, s_norm):
    n, block, width = lines.shape
    _, le, hidden = e_norm.shape
    cols = s_norm.shape[1]
    q = 3 * le * hidden // (4 * width)
    rows = []
    for c in range(2):
        for b in range(2):
            acc = lines[2 * b + c].astype(F32)
            for d in range(4 + 2 * b + c, n, 4):
                acc = acc + lines[d].astype(F32)
            rows.append(acc)
    whole = rows[0] + rows[1] + rows[2] + rows[3]
    rows = [r[i : i + 1] * scale for r in rows for i in range(q)]
    per = hidden // width
    for t in range(3):
        for e in range(le):
            at = (t * le + e) * per
            e_norm[t, e : e + 1, :] = jnp.concatenate(rows[at : at + per], 1)
    line = jnp.concatenate([whole[i : i + 1] for i in range(q, block)], 1) * scale
    for t in range(3):
        s_norm[t : t + 1, :] = line[:, t * cols : (t + 1) * cols]


def project(sizes, pos, got, both, *refs):
    weights, results = refs[:6], refs[6:10]
    xt_ref, gt_ref, xs_ref, gs_ref = refs[10:14]
    held, made = refs[14:20], refs[20:24]
    sem_in, sem_out = refs[24], refs[25]
    le, width, hidden = held[0].shape
    loads = [pltpu.make_async_copy(weights[k], held[k], sem_in.at[k]) for k in range(6)]
    for load in loads:
        load.start()
    nb, rows = got.shape[0], both.shape[0]
    sec = made[0].shape[0]
    half = 2 * sec
    z, c = pos[0], pos[1]
    src, kd, _, _ = ring_rows(along(2 * half, 0), z, c, sizes)
    cols = lax.broadcasted_iota(jnp.int32, (2 * half, nb), 1)
    mine = mm(one_hot(src, cols), got[...])
    mine = mine + mm(one_hot(src - nb, lax.broadcasted_iota(jnp.int32, (2 * half, rows), 1)), both[...])
    part = [jnp.where(kd == e, mine, 0.0).astype(BF) for e in range(le + 1)]
    x = jnp.concatenate([p[:, :width] for p in part[:le]], 1)
    g = jnp.concatenate([p[:, width:] for p in part[:le]], 1)
    stores = []
    for t, (xe, xs) in enumerate(((x, part[le][:, :width]), (x, part[le][:, :width]), (g, part[le][:, width:]))):
        cut = slice(t * hidden, (t + 1) * hidden)
        loads[t].wait()
        loads[3 + t].wait()
        p = mm(xe, held[t][...].reshape(le * width, hidden)) + mm(xs, held[3 + t][...])
        for k in (3, 1, 2, 0):
            at = (0, sec, half, half + sec)[k]
            made[k][:, cut] = p[at : at + sec].astype(made[k].dtype)
            store = pltpu.make_async_copy(made[k].at[:, cut], results[k].at[:, cut], sem_out.at[t, k])
            store.start()
            stores.append(store)
    _, kr, _, _ = ring_rows(along(2 * half, 1), z, c, sizes)
    mine_t = mine.T
    for e in range(le + 1):
        both_t = jnp.where(kr == e, mine_t, 0.0).astype(BF)
        to_x, to_g, at = (xt_ref, gt_ref, e * width) if e < le else (xs_ref, gs_ref, 0)
        to_x[at : at + width, :] = both_t[:width]
        to_g[at : at + width, :] = both_t[width:]
    for store in stores:
        store.wait()


def over_rows(lhs, parts, cut):
    at, out = 0, None
    for p in parts:
        n = p.shape[0]
        r = mm(lhs[:, at : at + n], p[:, cut])
        out = r if out is None else out + r
        at += n
    return out


def stack_rows(*refs):
    at, out = 0, refs[-1]
    for ref in refs[:-1]:
        out[at : at + ref.shape[0], :] = ref[...]
        at += ref.shape[0]


def expert_grads(g0, g1, g2, g3, xt, gt, after, stack, sq):
    _, le, width, hidden = stack.shape
    for t, lhs in enumerate((xt, xt, gt)):
        r = over_rows(lhs, (g0, g1, g2, g3), slice(t * hidden, (t + 1) * hidden)).reshape(le, width, hidden)
        stack[t] = r.astype(BF)
        total = jnp.sum(r * r, axis=1, keepdims=True)
        per = hidden // width
        for e in range(le):
            for q in range(per):
                at = (t * le + e) * per + q
                sq[at : at + 1, :] = total[e, :, q * width : (q + 1) * width]


def row_grads(sizes, pos, g0, g1, g2, g3, eg, eu, sg, su, xs, gs, out, shared):
    le, width, hidden = eg.shape
    ls, bl = sizes[2], sizes[4]
    n_ep, rows = out.shape[0], shared.shape[0]
    nb = n_ep * bl
    cols = hidden // n_ep
    for t, lhs in enumerate((xs, xs, gs)):
        r = over_rows(lhs, (g0, g1, g2, g3), slice(t * hidden, (t + 1) * hidden))
        out[:, t * cols : (t + 1) * cols, :] = r.T.astype(BF).reshape(n_ep, cols, width)
    total = 2 * sizes[0] * sizes[1]
    z, c = pos[0], pos[1]
    _, kd, _, within = ring_rows(along(total, 0), z, c, sizes)
    slots, wg, at = [], [], 0
    for src in (g0, g1, g2, g3):
        n = src.shape[0]
        gg, gu = src[:, :hidden], src[:, hidden : 2 * hidden]
        se = mm(gg, eg[...].reshape(le * width, hidden), NT) + mm(gu, eu[...].reshape(le * width, hidden), NT)
        ss = mm(gg, sg[...], NT) + mm(gu, su[...], NT)
        k = kd[at : at + n]
        s = jnp.where(k == le, ss, 0.0)
        for e in range(le):
            s = s + jnp.where(k == e, se[:, e * width : (e + 1) * width], 0.0)
        slots.append(s)
        lanes = lax.broadcasted_iota(jnp.int32, (n, width), 1)
        wg.append(jnp.where(within[at : at + n] == lanes, src[:, 3 * hidden :].astype(F32), 0.0))
        at += n
    slot = jnp.concatenate(slots, 0)
    hi = slot.astype(BF)
    rest = slot - hi.astype(F32)
    mid = rest.astype(BF)
    low = (rest - mid.astype(F32)).astype(BF)
    src_r, _, block, _ = ring_rows(along(total, 1), z, c, sizes)
    lines = lax.broadcasted_iota(jnp.int32, (nb, total), 0)
    to_slot = one_hot(lines, src_r)
    to_tail = one_hot(lines, jnp.where(block >= 0, block * bl + ls, -1))
    back = mm(to_slot, hi) + mm(to_tail, jnp.concatenate(wg, 0).astype(BF))
    out[:, 3 * cols :, :] = back.reshape(n_ep, bl, width).astype(BF)
    ps = one_hot(lax.broadcasted_iota(jnp.int32, (rows, total), 0) + nb, src_r)
    shared[...] = mm(ps, hi) + mm(ps, mid) + mm(ps, low)


def row_backward(summed, weights):
    hidden = summed.shape[1] // 3
    pre_gate = summed[:, :hidden]
    pre_up = summed[:, hidden : 2 * hidden]
    back_act = summed[:, 2 * hidden :]
    sigmoid_gate = jax.nn.sigmoid(pre_gate)
    silu_gate = pre_gate * sigmoid_gate
    activation = silu_gate * pre_up
    act_grad = weights * back_act
    grad_up = (act_grad * silu_gate).astype(BF)
    grad_gate = (act_grad * pre_up * sigmoid_gate * (1.0 + pre_gate * (1.0 - sigmoid_gate))).astype(BF)
    scaled_act = (weights * activation).astype(BF)
    weight_grad = jnp.sum(activation * back_act, axis=1, keepdims=True).astype(BF)
    return grad_gate, grad_up, scaled_act, weight_grad


def body(tokens, cotangent, routes, gate_weights, e_gate, e_up, e_down, s_gate, s_up, s_down):
    n_ep, n_tp = lax.axis_size("ep"), lax.axis_size("tp")
    nz = n_tp // 2
    rows, width = tokens.shape
    top = routes.shape[1]
    le, _, hidden = e_gate.shape
    experts = le * n_ep
    cap = 3 * rows * top // (2 * experts)
    ls = le * cap
    bl = (ls + 8) // 8 * 8
    slots = n_ep * ls
    total = slots + rows
    piece = total // n_tp
    tp = lax.axis_index("tp")
    z, c = tp // 2, tp % 2
    fwd = [(i, (i + 4 - 8 * (i % 2)) % n_tp) for i in range(n_tp)]
    bwd = [(b, a) for a, b in fwd]
    pair = [(i, (2 * ((i // 2 + i % 2) % nz ^ 1) - i % 2) % n_tp) for i in range(n_tp)]
    swap = [(i, i ^ 1) for i in range(n_tp)]

    geo = (le, cap, experts, bl)
    lanes = jnp.arange(2 * width, dtype=jnp.int32)
    groups = jnp.arange(n_ep, dtype=jnp.int32)
    sent, both = call(
        functools.partial(dispatch, geo),
        [((n_ep * bl, 2 * width), BF), ((rows, 2 * width), BF)],
        tokens, cotangent, routes.T, gate_weights.T,
    )
    got = lax.all_to_all(sent.reshape(n_ep, bl, 2 * width), "ep", 0, 0, tiled=True)

    sizes = (nz, piece, ls, cap, bl, slots)
    pos = jnp.stack([z, c]).astype(jnp.int32)
    members = nz // 2
    hops, back_hops = members // 2, members - members // 2 - 1
    sec = members * piece
    width3 = 3 * hidden
    big = [((sec, width3), F32)] * 2 + [((sec, width3), BF)] * 2
    turned = [((le * width, total), BF)] * 2 + [((width, total), BF)] * 2
    weights = (e_gate, e_up, e_down, s_gate, s_up, s_down)
    anywhere = pl.BlockSpec(memory_space=pl.ANY)
    own_k, own_s, out_k, out_s, xt, gt, xs, gs = pl.pallas_call(
        functools.partial(project, sizes),
        out_shape=[jax.ShapeDtypeStruct(a, d) for a, d in big + turned],
        in_specs=[pl.BlockSpec(memory_space=pltpu.SMEM), VM, VM] + [anywhere] * 6,
        out_specs=[anywhere] * 4 + [VM] * 4,
        scratch_shapes=[pltpu.VMEM(w.shape, BF) for w in weights]
        + [pltpu.VMEM(a, d) for a, d in big]
        + [pltpu.SemaphoreType.DMA((6,)), pltpu.SemaphoreType.DMA((3, 4))],
    )(pos, got.reshape(n_ep * bl, 2 * width), both, *weights)
    oth_s = lax.ppermute(out_s, "tp", swap)
    oth_k = lax.ppermute(out_k, "tp", swap)
    cut = 2 * piece
    to_a = (own_s[:cut] + oth_s[:cut].astype(F32)).astype(BF)
    to_b = (own_s[cut:] + oth_s[cut:].astype(F32)).astype(BF)
    par_a = lax.ppermute(to_a, "tp", pair)
    par_b = lax.ppermute(to_b, "tp", pair)
    left_rows = slice(cut, hops * piece)
    on_left = lax.optimization_barrier((own_k[left_rows], oth_k[left_rows], par_b[: hops * piece - cut]))

    def at(m):
        p = (m - hops) % members
        rows_p = slice(p * piece, (p + 1) * piece)
        par = par_a[rows_p] if p < 2 else par_b[p * piece - cut : (p + 1) * piece - cut]
        own, oth = own_k, oth_k
        if 1 < p < hops:
            (own, oth, par), rows_p = on_left, slice((p - 2) * piece, (p - 1) * piece)
            par = par[rows_p]
        return own[rows_p] + oth[rows_p].astype(F32) + par.astype(F32)

    right, left = at(hops).astype(BF), at(hops + 1).astype(BF)
    for t in range(hops):
        right = lax.ppermute(right, "tp", fwd)
        if t < hops - 1:
            right = (right.astype(F32) + at(hops - 1 - t)).astype(BF)
        if t < back_hops:
            left = lax.ppermute(left, "tp", bwd)
        if t < back_hops - 1:
            left = (left.astype(F32) + at(hops + 2 + t)).astype(BF)
    summed = right.astype(F32) + left.astype(F32) + at(0)

    q = tp * piece + jnp.arange(piece, dtype=jnp.int32)
    w_rows = mm(hot((q // ls)[:, None], groups[None, :]), got[:, ls, :])
    own_w = jnp.sum(jnp.where((q % ls)[:, None] == lanes[None, :], w_rows, 0.0), axis=1)
    own_w = jnp.where(q < slots, own_w, 1.0)[:, None]
    gg, gu, sa, wg = row_backward(summed, own_w)
    block = jnp.concatenate([gg, gu, sa, jnp.broadcast_to(wg, (piece, 128))], 1)

    ring = [None] * members
    ring[0] = right = left = block
    for t in range(1, hops + 1):
        right = lax.ppermute(right, "tp", fwd)
        ring[-t % members] = right
        if t <= back_hops:
            left = lax.ppermute(left, "tp", bwd)
            ring[t] = left
    parts = ring[hops + 1 :] + ring[:hops]
    (most,) = call(stack_rows, [((len(parts) * piece, block.shape[1]), BF)], *parts, limit=8 * 2**20)
    most_o = lax.ppermute(most, "tp", pair)
    last_o = lax.ppermute(ring[hops], "tp", pair)
    kept = jnp.concatenate([ring[hops], most], 0)
    kept_x = lax.ppermute(kept, "tp", swap)
    paired = jnp.concatenate([last_o, most_o], 0)
    paired_x = lax.ppermute(paired, "tp", swap)
    grads = (kept, paired, kept_x, paired_x)

    cols = hidden // n_ep
    out, shared_part = call(
        functools.partial(row_grads, sizes),
        [((n_ep, 3 * cols + bl, width), BF), ((rows, width), F32)],
        pos, *grads, e_gate, e_up, s_gate, s_up, xs, gs, smem=1,
    )
    home = lax.all_to_all(out, "ep", 0, 0, tiled=True)
    stack, e_sq = call(
        expert_grads, [((3, le, width, hidden), BF), ((3 * le * hidden // width, width), F32)], *grads, xt, gt, out, rest=1
    )
    e_sq = e_sq.reshape(2, -1, width)
    other_sq = lax.ppermute(jnp.where(c == 0, e_sq[1], e_sq[0]), "tp", swap)
    e_sq = (jnp.where(c == 0, e_sq[0], e_sq[1]) + other_sq).reshape(2, -1, width)
    other_sq = lax.ppermute(jnp.where(z % 2 == 0, e_sq[1], e_sq[0]), "tp", [(i, i ^ 2) for i in range(n_tp)])
    e_sq = jnp.where(z % 2 == 0, e_sq[0], e_sq[1]) + other_sq
    n_lines = (e_sq.shape[0] + -(-3 * cols // width) + 15) // 16 * 16
    shared, lines = call(
        gather_norms, [((3, cols, width), F32), ((n_tp, n_lines, width), BF)], home, e_sq
    )
    got_lines = lax.all_to_all(lines, "tp", 0, 0, tiled=True)
    token_grad, gate_grad = call(
        functools.partial(collect, geo),
        [((rows, width), BF), ((top, rows), F32)],
        home, shared_part, routes.T, lines, rest=1,
    )
    e_norm, s_norm = call(
        functools.partial(finish_norms, 1.0 / (width * n_tp)),
        [((3, le, hidden), F32), ((3, cols), F32)],
        got_lines,
    )
    return token_grad, gate_grad.astype(BF).T, stack, jnp.swapaxes(shared, 1, 2), e_norm, s_norm


def solution(mesh):
    return jax.shard_map(
        body,
        mesh=mesh,
        in_specs=(
            P("ep", "tp"),
            P("ep", "tp"),
            P("ep", None),
            P("ep", None),
            P("ep", "tp", None),
            P("ep", "tp", None),
            P("ep", "tp", None),
            P("tp", None),
            P("tp", None),
            P("tp", None),
        ),
        out_specs=(
            P("ep", "tp"),
            P("ep", None),
            P(None, "ep", "tp", None),
            P(None, "tp", "ep"),
            P(None, "ep", None),
            P(None, "ep"),
        ),
        check_vma=False,
    )
```

```python
import functools

import jax
import jax.numpy as jnp
from jax import lax
from jax.experimental import pallas as pl
from jax.experimental.pallas import tpu as pltpu
from jax.sharding import PartitionSpec as P


BF = jnp.bfloat16
F32 = jnp.float32
VM = pl.BlockSpec(memory_space=pltpu.VMEM)


def mm(a, b, dims=((1,), (0,))):
    return lax.dot_general(a, b, (dims, ((), ())), preferred_element_type=F32)


NT = ((1,), (1,))


def hot(a, b):
    return (a == b).astype(BF)


def call(kernel, outs, *args, smem=0, rest=0, limit=None):
    first = [pl.BlockSpec(memory_space=pltpu.SMEM)] * smem
    last = [pl.BlockSpec(memory_space=pl.ANY)] * rest
    return pl.pallas_call(
        kernel,
        out_shape=[jax.ShapeDtypeStruct(s, d) for s, d in outs],
        in_specs=first + [VM] * (len(args) - smem - rest) + last,
        out_specs=[VM] * len(outs),
        compiler_params=pltpu.CompilerParams(vmem_limit_bytes=limit),
    )(*args)


def quotient(n, by, top):
    shift = 0
    while (1 << shift) < by * top:
        shift += 1
    factor = -(-(1 << shift) // by)
    assert factor * top < 2**31
    return lax.shift_right_logical(n * factor, jnp.int32(shift))


def ring_rows(r, z, c, sizes):
    nz, piece, ls, cap, bl, slots = sizes
    sec = nz // 2 * piece
    half = 2 * sec
    h = (r >= half).astype(jnp.int32)
    inner = r - half * h
    q = (inner >= sec).astype(jnp.int32)
    inner = inner - sec * q
    m = quotient(inner, piece, sec)
    core = jnp.abs(c - h)
    zeta = (z + core) & (nz - 1)
    zeta = zeta + q * (1 - 2 * (zeta & 1)) + 2 * (1 - 2 * core) * (m + nz // 4)
    place = piece * (2 * ((zeta - core) & (nz - 1)) + core) + inner - piece * m
    block = quotient(place, ls, 2 * half)
    within = place - ls * block
    routed = place < slots
    expert = jnp.where(routed, quotient(within, cap, ls), ls // cap)
    src = jnp.where(routed, block * bl + within, slots // ls * bl + place - slots)
    return src, expert, jnp.where(routed, block, -1), within


def along(n, dim):
    return lax.broadcasted_iota(jnp.int32, (n, 1) if dim == 0 else (1, n), dim)


def one_hot(a, b):
    return jnp.where(a == b, 1.0, 0.0).astype(BF)


def columns(lines):
    lines = lines.astype(F32)
    return jnp.concatenate([lines, jnp.zeros((8 - lines.shape[0], lines.shape[1]), F32)], 0).T


def routing(routes, le, cap, experts):
    top, rows = routes.shape
    routes = columns(routes).astype(jnp.int32)
    lanes = lax.broadcasted_iota(jnp.int32, (rows, experts), 1)
    chosen = [routes[:, k : k + 1] for k in range(top)]
    on = [jnp.where(f == lanes, 1.0, 0.0) for f in chosen]
    shape = (rows, rows)
    tri = jnp.where(lax.broadcasted_iota(jnp.int32, shape, 0) > lax.broadcasted_iota(jnp.int32, shape, 1), 1.0, 0.0)
    before = mm(tri.astype(BF), sum(on).astype(BF))
    out = []
    for f, o in zip(chosen, on):
        dest = quotient(f, le, experts)
        pos = jnp.sum(o * before, axis=1, keepdims=True).astype(jnp.int32)
        out.append((dest, (f - le * dest) * cap + pos))
    return out


def dispatch(geo, tokens, cotangent, routes, weights, sent, both):
    le, cap, experts, bl = geo
    rows, width = tokens.shape
    n = sent.shape[0]
    xg = jnp.concatenate([tokens[...], cotangent[...]], 1)
    both[...] = xg
    where = routing(routes[...], le, cap, experts)
    cols = lax.broadcasted_iota(jnp.int32, (rows, n), 1)
    lanes = lax.broadcasted_iota(jnp.int32, (rows, 2 * width), 1)
    w = columns(weights[...])
    left, right = [jnp.zeros((rows, n), F32)], [xg]
    for k, (dest, within) in enumerate(where):
        left[0] = left[0] + jnp.where(dest * bl + within == cols, 1.0, 0.0)
        left.append(jnp.where(dest * bl + le * cap == cols, w[:, k : k + 1], 0.0))
        right.append(one_hot(within, lanes))
    left = jnp.concatenate([a.T.astype(BF) for a in left], 1)
    sent[...] = mm(left, jnp.concatenate(right, 0)).astype(BF)


def collect(geo, home, shared, routes, after, token_grad, gate_grad):
    le, cap, experts, bl = geo
    n_ep = home.shape[0]
    rows, width = shared.shape
    n = n_ep * bl
    first = home.shape[1] - bl
    where = routing(routes[...], le, cap, experts)
    cols = lax.broadcasted_iota(jnp.int32, (rows, n), 1)
    lanes = lax.broadcasted_iota(jnp.int32, (rows, width), 1)
    back = home[:, first:, :].astype(F32).reshape(n, width).astype(BF)
    pick, picked = jnp.zeros((rows, n), F32), []
    for dest, within in where:
        pick = pick + jnp.where(dest * bl + within == cols, 1.0, 0.0)
        line = mm(one_hot(dest * bl + le * cap, cols), back)
        picked.append(jnp.sum(jnp.where(within == lanes, line, 0.0), axis=1, keepdims=True))
    picked.append(jnp.zeros((rows, 8 - len(picked)), F32))
    gate_grad[...] = jnp.concatenate(picked, 1).T[: gate_grad.shape[0]]
    token_grad[...] = (mm(pick.astype(BF), back) + shared[...]).astype(BF)


def gather_norms(home, quarter, shared, lines):
    _, cols, width = shared.shape
    hidden_rows = 3 * cols
    acc = home[0, :hidden_rows, :].astype(F32)
    for e in range(1, home.shape[0]):
        acc = acc + home[e, :hidden_rows, :].astype(F32)
    turned = acc.T
    for t in range(3):
        shared[t] = acc[t * cols : (t + 1) * cols]
    row = jnp.sum(turned * turned, axis=0, keepdims=True)
    fill = lines.shape[1] * width - quarter.shape[0] * width - hidden_rows
    row = jnp.concatenate([row, jnp.zeros((1, fill), F32)], 1)
    parts = [quarter[...]] + [row[:, a : a + width] for a in range(0, row.shape[1], width)]
    lines[...] = jnp.broadcast_to(jnp.concatenate(parts, 0).astype(BF)[None], lines.shape)


def finish_norms(scale, pos, lines, other, e_norm, s_norm):
    n, block, width = lines.shape
    _, le, hidden = e_norm.shape
    cols = s_norm.shape[1]
    q = 3 * le * hidden // (4 * width)
    c = pos[1]
    sums = []
    for ref in (lines, other):
        for b in range(2):
            acc = ref[b].astype(F32)
            for d in range(2 + b, n, 2):
                acc = acc + ref[d].astype(F32)
            sums.append(acc)
    rows = [jnp.where(c == 0, sums[k], sums[(k + 2) % 4]) for k in range(4)]
    whole = rows[0] + rows[1] + rows[2] + rows[3]
    rows = [r[i : i + 1] * scale for r in rows for i in range(q)]
    per = hidden // width
    for t in range(3):
        for e in range(le):
            at = (t * le + e) * per
            e_norm[t, e : e + 1, :] = jnp.concatenate(rows[at : at + per], 1)
    line = jnp.concatenate([whole[i : i + 1] for i in range(q, block)], 1) * scale
    for t in range(3):
        s_norm[t : t + 1, :] = line[:, t * cols : (t + 1) * cols]


def project(sizes, pos, got, both, *refs):
    weights, results = refs[:6], refs[6:10]
    xt_ref, gt_ref, xs_ref, gs_ref = refs[10:14]
    held, made = refs[14:17], refs[17:21]
    sem_in, sem_out = refs[21], refs[22]
    le, width, hidden = weights[0].shape
    loads = []
    for t in range(3):
        for e in range(le + 1):
            src = weights[t].at[e] if e < le else weights[3 + t]
            to = held[t].at[e * width : (e + 1) * width, :]
            loads.append(pltpu.make_async_copy(src, to, sem_in.at[t, e]))
            loads[-1].start()
    nb, rows = got.shape[0], both.shape[0]
    sec = made[0].shape[0]
    half = 2 * sec
    z, c = pos[0], pos[1]
    src, kd, _, _ = ring_rows(along(2 * half, 0), z, c, sizes)
    cols = lax.broadcasted_iota(jnp.int32, (2 * half, nb), 1)
    mine = mm(one_hot(src, cols), got[...])
    mine = mine + mm(one_hot(src - nb, lax.broadcasted_iota(jnp.int32, (2 * half, rows), 1)), both[...])
    part = [jnp.where(kd == e, mine, 0.0).astype(BF) for e in range(le + 1)]
    x = jnp.concatenate([p[:, :width] for p in part], 1)
    g = jnp.concatenate([p[:, width:] for p in part], 1)
    stores = []
    for t, lhs in enumerate((x, x, g)):
        cut = slice(t * hidden, (t + 1) * hidden)
        for load in loads[t * (le + 1) : (t + 1) * (le + 1)]:
            load.wait()
        p = mm(lhs, held[t][...])
        for k in (3, 1, 2, 0):
            at = (0, sec, half, half + sec)[k]
            made[k][:, cut] = p[at : at + sec].astype(made[k].dtype)
            store = pltpu.make_async_copy(made[k].at[:, cut], results[k].at[:, cut], sem_out.at[t, k])
            store.start()
            stores.append(store)
    _, kr, _, _ = ring_rows(along(2 * half, 1), z, c, sizes)
    mine_t = mine.T
    for e in range(le + 1):
        both_t = jnp.where(kr == e, mine_t, 0.0).astype(BF)
        to_x, to_g, at = (xt_ref, gt_ref, e * width) if e < le else (xs_ref, gs_ref, 0)
        to_x[at : at + width, :] = both_t[:width]
        to_g[at : at + width, :] = both_t[width:]
    for store in stores:
        store.wait()


def over_rows(lhs, parts, cut):
    at, out = 0, None
    for p in parts:
        n = p.shape[0]
        r = mm(lhs[:, at : at + n], p[:, cut])
        out = r if out is None else out + r
        at += n
    return out


def stack_rows(*refs):
    at, out = 0, refs[-1]
    for ref in refs[:-1]:
        out[at : at + ref.shape[0], :] = ref[...]
        at += ref.shape[0]


def expert_grads(g0, g1, g2, g3, xt, gt, after, stack, sq):
    _, le, width, hidden = stack.shape
    for t, lhs in enumerate((xt, xt, gt)):
        r = over_rows(lhs, (g0, g1, g2, g3), slice(t * hidden, (t + 1) * hidden)).reshape(le, width, hidden)
        stack[t] = r.astype(BF)
        total = jnp.sum(r * r, axis=1, keepdims=True)
        per = hidden // width
        for e in range(le):
            for q in range(per):
                at = (t * le + e) * per + q
                sq[at : at + 1, :] = total[e, :, q * width : (q + 1) * width]


def row_grads(sizes, pos, g0, g1, g2, g3, eg, eu, sg, su, xs, gs, out, shared):
    le, width, hidden = eg.shape
    ls, bl = sizes[2], sizes[4]
    n_ep, rows = out.shape[0], shared.shape[0]
    nb = n_ep * bl
    cols = hidden // n_ep
    for t, lhs in enumerate((xs, xs, gs)):
        r = over_rows(lhs, (g0, g1, g2, g3), slice(t * hidden, (t + 1) * hidden))
        out[:, t * cols : (t + 1) * cols, :] = r.T.astype(BF).reshape(n_ep, cols, width)
    total = 2 * sizes[0] * sizes[1]
    z, c = pos[0], pos[1]
    _, kd, _, within = ring_rows(along(total, 0), z, c, sizes)
    slots, wg, at = [], [], 0
    for src in (g0, g1, g2, g3):
        n = src.shape[0]
        gg, gu = src[:, :hidden], src[:, hidden : 2 * hidden]
        se = mm(gg, eg[...].reshape(le * width, hidden), NT) + mm(gu, eu[...].reshape(le * width, hidden), NT)
        ss = mm(gg, sg[...], NT) + mm(gu, su[...], NT)
        k = kd[at : at + n]
        s = jnp.where(k == le, ss, 0.0)
        for e in range(le):
            s = s + jnp.where(k == e, se[:, e * width : (e + 1) * width], 0.0)
        slots.append(s)
        lanes = lax.broadcasted_iota(jnp.int32, (n, width), 1)
        wg.append(jnp.where(within[at : at + n] == lanes, src[:, 3 * hidden :].astype(F32), 0.0))
        at += n
    slot = jnp.concatenate(slots, 0)
    hi = slot.astype(BF)
    rest = slot - hi.astype(F32)
    mid = rest.astype(BF)
    low = (rest - mid.astype(F32)).astype(BF)
    src_r, _, block, _ = ring_rows(along(total, 1), z, c, sizes)
    lines = lax.broadcasted_iota(jnp.int32, (nb, total), 0)
    to_slot = one_hot(lines, src_r)
    to_tail = one_hot(lines, jnp.where(block >= 0, block * bl + ls, -1))
    back = mm(to_slot, hi) + mm(to_tail, jnp.concatenate(wg, 0).astype(BF))
    out[:, 3 * cols :, :] = back.reshape(n_ep, bl, width).astype(BF)
    ps = one_hot(lax.broadcasted_iota(jnp.int32, (rows, total), 0) + nb, src_r)
    shared[...] = mm(ps, hi) + mm(ps, mid) + mm(ps, low)


def row_backward(summed, weights):
    hidden = summed.shape[1] // 3
    pre_gate = summed[:, :hidden]
    pre_up = summed[:, hidden : 2 * hidden]
    back_act = summed[:, 2 * hidden :]
    sigmoid_gate = jax.nn.sigmoid(pre_gate)
    silu_gate = pre_gate * sigmoid_gate
    activation = silu_gate * pre_up
    act_grad = weights * back_act
    grad_up = (act_grad * silu_gate).astype(BF)
    grad_gate = (act_grad * pre_up * sigmoid_gate * (1.0 + pre_gate * (1.0 - sigmoid_gate))).astype(BF)
    scaled_act = (weights * activation).astype(BF)
    weight_grad = jnp.sum(activation * back_act, axis=1, keepdims=True).astype(BF)
    return grad_gate, grad_up, scaled_act, weight_grad


def body(tokens, cotangent, routes, gate_weights, e_gate, e_up, e_down, s_gate, s_up, s_down):
    n_ep, n_tp = lax.axis_size("ep"), lax.axis_size("tp")
    nz = n_tp // 2
    rows, width = tokens.shape
    top = routes.shape[1]
    le, _, hidden = e_gate.shape
    experts = le * n_ep
    cap = 3 * rows * top // (2 * experts)
    ls = le * cap
    bl = (ls + 8) // 8 * 8
    slots = n_ep * ls
    total = slots + rows
    piece = total // n_tp
    tp = lax.axis_index("tp")
    z, c = tp // 2, tp % 2
    fwd = [(i, (i + 4 - 8 * (i % 2)) % n_tp) for i in range(n_tp)]
    bwd = [(b, a) for a, b in fwd]
    pair = [(i, (2 * ((i // 2 + i % 2) % nz ^ 1) - i % 2) % n_tp) for i in range(n_tp)]
    swap = [(i, i ^ 1) for i in range(n_tp)]

    geo = (le, cap, experts, bl)
    lanes = jnp.arange(2 * width, dtype=jnp.int32)
    groups = jnp.arange(n_ep, dtype=jnp.int32)
    sent, both = call(
        functools.partial(dispatch, geo),
        [((n_ep * bl, 2 * width), BF), ((rows, 2 * width), BF)],
        tokens, cotangent, routes.T, gate_weights.T,
    )
    got = lax.all_to_all(sent.reshape(n_ep, bl, 2 * width), "ep", 0, 0, tiled=True)

    sizes = (nz, piece, ls, cap, bl, slots)
    pos = jnp.stack([z, c]).astype(jnp.int32)
    members = nz // 2
    hops, back_hops = members // 2, members - members // 2 - 1
    sec = members * piece
    width3 = 3 * hidden
    big = [((sec, width3), F32)] * 2 + [((sec, width3), BF)] * 2
    turned = [((le * width, total), BF)] * 2 + [((width, total), BF)] * 2
    weights = (e_gate, e_up, e_down, s_gate, s_up, s_down)
    anywhere = pl.BlockSpec(memory_space=pl.ANY)
    own_k, own_s, out_k, out_s, xt, gt, xs, gs = pl.pallas_call(
        functools.partial(project, sizes),
        out_shape=[jax.ShapeDtypeStruct(a, d) for a, d in big + turned],
        in_specs=[pl.BlockSpec(memory_space=pltpu.SMEM), VM, VM] + [anywhere] * 6,
        out_specs=[anywhere] * 4 + [VM] * 4,
        scratch_shapes=[pltpu.VMEM(((le + 1) * width, hidden), BF)] * 3
        + [pltpu.VMEM(a, d) for a, d in big]
        + [pltpu.SemaphoreType.DMA((3, le + 1)), pltpu.SemaphoreType.DMA((3, 4))],
    )(pos, got.reshape(n_ep * bl, 2 * width), both, *weights)
    oth_s = lax.ppermute(out_s, "tp", swap)
    oth_k = lax.ppermute(out_k, "tp", swap)
    cut = (hops + 1) * piece
    to_a = (own_s[:cut] + oth_s[:cut].astype(F32)).astype(BF)
    to_b = (own_s[cut:] + oth_s[cut:].astype(F32)).astype(BF)
    par_a = lax.ppermute(to_a, "tp", pair)
    par_b = lax.ppermute(to_b, "tp", pair)
    left_rows = slice(2 * piece, hops * piece)
    on_left = lax.optimization_barrier((own_k[left_rows], oth_k[left_rows], par_a[left_rows]))

    def at(m):
        p = (m - hops) % members
        rows_p = slice(p * piece, (p + 1) * piece)
        par = par_a[rows_p] if p <= hops else par_b[p * piece - cut : (p + 1) * piece - cut]
        own, oth = own_k, oth_k
        if 1 < p < hops:
            (own, oth, par), rows_p = on_left, slice((p - 2) * piece, (p - 1) * piece)
            par = par[rows_p]
        return own[rows_p] + oth[rows_p].astype(F32) + par.astype(F32)

    right, left = at(hops).astype(BF), at(hops + 1).astype(BF)
    for t in range(hops):
        right = lax.ppermute(right, "tp", fwd)
        if t < hops - 1:
            right = (right.astype(F32) + at(hops - 1 - t)).astype(BF)
        if t < back_hops:
            left = lax.ppermute(left, "tp", bwd)
        if t < back_hops - 1:
            left = (left.astype(F32) + at(hops + 2 + t)).astype(BF)
    summed = right.astype(F32) + left.astype(F32) + at(0)

    q = tp * piece + jnp.arange(piece, dtype=jnp.int32)
    w_rows = mm(hot((q // ls)[:, None], groups[None, :]), got[:, ls, :])
    own_w = jnp.sum(jnp.where((q % ls)[:, None] == lanes[None, :], w_rows, 0.0), axis=1)
    own_w = jnp.where(q < slots, own_w, 1.0)[:, None]
    gg, gu, sa, wg = row_backward(summed, own_w)
    block = jnp.concatenate([gg, gu, sa, jnp.broadcast_to(wg, (piece, 128))], 1)

    ring = [None] * members
    ring[0] = right = left = block
    for t in range(1, hops + 1):
        right = lax.ppermute(right, "tp", fwd)
        ring[-t % members] = right
        if t <= back_hops:
            left = lax.ppermute(left, "tp", bwd)
            ring[t] = left
    parts = ring[hops + 1 :] + ring[:hops]
    (most,) = call(stack_rows, [((len(parts) * piece, block.shape[1]), BF)], *parts, limit=8 * 2**20)
    most_o = lax.ppermute(most, "tp", pair)
    last_o = lax.ppermute(ring[hops], "tp", pair)
    kept = jnp.concatenate([ring[hops], most], 0)
    kept_x = lax.ppermute(kept, "tp", swap)
    paired = jnp.concatenate([last_o, most_o], 0)
    paired_x = lax.ppermute(paired, "tp", swap)
    grads = (kept, paired, kept_x, paired_x)

    cols = hidden // n_ep
    out, shared_part = call(
        functools.partial(row_grads, sizes),
        [((n_ep, 3 * cols + bl, width), BF), ((rows, width), F32)],
        pos, *grads, e_gate, e_up, s_gate, s_up, xs, gs, smem=1,
    )
    home = lax.all_to_all(out, "ep", 0, 0, tiled=True)
    stack, e_sq = call(
        expert_grads, [((3, le, width, hidden), BF), ((3 * le * hidden // width, width), F32)], *grads, xt, gt, out, rest=1
    )
    e_sq = e_sq.reshape(2, -1, width)
    other_sq = lax.ppermute(jnp.where(c == 0, e_sq[1], e_sq[0]), "tp", swap)
    e_sq = (jnp.where(c == 0, e_sq[0], e_sq[1]) + other_sq).reshape(2, -1, width)
    other_sq = lax.ppermute(jnp.where(z % 2 == 0, e_sq[1], e_sq[0]), "tp", [(i, i ^ 2) for i in range(n_tp)])
    e_sq = jnp.where(z % 2 == 0, e_sq[0], e_sq[1]) + other_sq
    n_lines = (e_sq.shape[0] + -(-3 * cols // width) + 15) // 16 * 16
    shared, lines = call(
        gather_norms, [((3, cols, width), F32), ((nz, n_lines, width), BF)], home, e_sq
    )
    same_core = [[2 * i + k for i in range(nz)] for k in range(2)]
    got_lines = lax.all_to_all(lines, "tp", 0, 0, axis_index_groups=same_core, tiled=True)
    token_grad, gate_grad = call(
        functools.partial(collect, geo),
        [((rows, width), BF), ((top, rows), F32)],
        home, shared_part, routes.T, lines, rest=1,
    )
    other_lines = lax.ppermute(got_lines, "tp", swap)
    e_norm, s_norm = call(
        functools.partial(finish_norms, 1.0 / (width * n_tp)),
        [((3, le, hidden), F32), ((3, cols), F32)],
        pos, got_lines, other_lines, smem=1,
    )
    return token_grad, gate_grad.astype(BF).T, stack, jnp.swapaxes(shared, 1, 2), e_norm, s_norm


def solution(mesh):
    return jax.shard_map(
        body,
        mesh=mesh,
        in_specs=(
            P("ep", "tp"),
            P("ep", "tp"),
            P("ep", None),
            P("ep", None),
            P("ep", "tp", None),
            P("ep", "tp", None),
            P("ep", "tp", None),
            P("tp", None),
            P("tp", None),
            P("tp", None),
        ),
        out_specs=(
            P("ep", "tp"),
            P("ep", None),
            P(None, "ep", "tp", None),
            P(None, "tp", "ep"),
            P(None, "ep", None),
            P(None, "ep"),
        ),
        check_vma=False,
    )
```

```python
import functools

import jax
import jax.numpy as jnp
from jax import lax
from jax.experimental import pallas as pl
from jax.experimental.pallas import tpu as pltpu
from jax.sharding import PartitionSpec as P


BF = jnp.bfloat16
F32 = jnp.float32
VM = pl.BlockSpec(memory_space=pltpu.VMEM)


def mm(a, b, dims=((1,), (0,))):
    return lax.dot_general(a, b, (dims, ((), ())), preferred_element_type=F32)


NT = ((1,), (1,))


def hot(a, b):
    return (a == b).astype(BF)


def call(kernel, outs, *args, smem=0, rest=0, limit=None):
    first = [pl.BlockSpec(memory_space=pltpu.SMEM)] * smem
    last = [pl.BlockSpec(memory_space=pl.ANY)] * rest
    return pl.pallas_call(
        kernel,
        out_shape=[jax.ShapeDtypeStruct(s, d) for s, d in outs],
        in_specs=first + [VM] * (len(args) - smem - rest) + last,
        out_specs=[VM] * len(outs),
        compiler_params=pltpu.CompilerParams(vmem_limit_bytes=limit),
    )(*args)


def quotient(n, by, top):
    shift = 0
    while (1 << shift) < by * top:
        shift += 1
    factor = -(-(1 << shift) // by)
    assert factor * top < 2**31
    return lax.shift_right_logical(n * factor, jnp.int32(shift))


def ring_rows(r, z, c, sizes):
    nz, piece, ls, cap, bl, slots = sizes
    sec = nz // 2 * piece
    half = 2 * sec
    h = (r >= half).astype(jnp.int32)
    inner = r - half * h
    q = (inner >= sec).astype(jnp.int32)
    inner = inner - sec * q
    m = quotient(inner, piece, sec)
    core = jnp.abs(c - h)
    zeta = (z + core) & (nz - 1)
    zeta = zeta + q * (1 - 2 * (zeta & 1)) + 2 * (1 - 2 * core) * (m + nz // 4)
    place = piece * (2 * ((zeta - core) & (nz - 1)) + core) + inner - piece * m
    block = quotient(place, ls, 2 * half)
    within = place - ls * block
    routed = place < slots
    expert = jnp.where(routed, quotient(within, cap, ls), ls // cap)
    src = jnp.where(routed, block * bl + within, slots // ls * bl + place - slots)
    return src, expert, jnp.where(routed, block, -1), within


def along(n, dim):
    return lax.broadcasted_iota(jnp.int32, (n, 1) if dim == 0 else (1, n), dim)


def one_hot(a, b):
    return jnp.where(a == b, 1.0, 0.0).astype(BF)


def columns(lines):
    lines = lines.astype(F32)
    return jnp.concatenate([lines, jnp.zeros((8 - lines.shape[0], lines.shape[1]), F32)], 0).T


def routing(routes, le, cap, experts):
    top, rows = routes.shape
    routes = columns(routes).astype(jnp.int32)
    lanes = lax.broadcasted_iota(jnp.int32, (rows, experts), 1)
    chosen = [routes[:, k : k + 1] for k in range(top)]
    on = [jnp.where(f == lanes, 1.0, 0.0) for f in chosen]
    shape = (rows, rows)
    tri = jnp.where(lax.broadcasted_iota(jnp.int32, shape, 0) > lax.broadcasted_iota(jnp.int32, shape, 1), 1.0, 0.0)
    before = mm(tri.astype(BF), sum(on).astype(BF))
    out = []
    for f, o in zip(chosen, on):
        dest = quotient(f, le, experts)
        pos = jnp.sum(o * before, axis=1, keepdims=True).astype(jnp.int32)
        out.append((dest, (f - le * dest) * cap + pos))
    return out


def dispatch(geo, tokens, cotangent, routes, weights, sent, both):
    le, cap, experts, bl = geo
    rows, width = tokens.shape
    n = sent.shape[0]
    xg = jnp.concatenate([tokens[...], cotangent[...]], 1)
    both[...] = xg
    where = routing(routes[...], le, cap, experts)
    cols = lax.broadcasted_iota(jnp.int32, (rows, n), 1)
    lanes = lax.broadcasted_iota(jnp.int32, (rows, 2 * width), 1)
    w = columns(weights[...])
    left, right = [jnp.zeros((rows, n), F32)], [xg]
    for k, (dest, within) in enumerate(where):
        left[0] = left[0] + jnp.where(dest * bl + within == cols, 1.0, 0.0)
        left.append(jnp.where(dest * bl + le * cap == cols, w[:, k : k + 1], 0.0))
        right.append(one_hot(within, lanes))
    left = jnp.concatenate([a.T.astype(BF) for a in left], 1)
    sent[...] = mm(left, jnp.concatenate(right, 0)).astype(BF)


def collect(geo, home, shared, routes, after, token_grad, gate_grad):
    le, cap, experts, bl = geo
    n_ep = home.shape[0]
    rows, width = shared.shape
    n = n_ep * bl
    first = home.shape[1] - bl
    where = routing(routes[...], le, cap, experts)
    cols = lax.broadcasted_iota(jnp.int32, (rows, n), 1)
    lanes = lax.broadcasted_iota(jnp.int32, (rows, width), 1)
    back = home[:, first:, :].astype(F32).reshape(n, width).astype(BF)
    pick, picked = jnp.zeros((rows, n), F32), []
    for dest, within in where:
        pick = pick + jnp.where(dest * bl + within == cols, 1.0, 0.0)
        line = mm(one_hot(dest * bl + le * cap, cols), back)
        picked.append(jnp.sum(jnp.where(within == lanes, line, 0.0), axis=1, keepdims=True))
    picked.append(jnp.zeros((rows, 8 - len(picked)), F32))
    gate_grad[...] = jnp.concatenate(picked, 1).T[: gate_grad.shape[0]]
    token_grad[...] = (mm(pick.astype(BF), back) + shared[...]).astype(BF)


def gather_norms(home, quarter, shared, lines):
    _, cols, width = shared.shape
    hidden_rows = 3 * cols
    acc = home[0, :hidden_rows, :].astype(F32)
    for e in range(1, home.shape[0]):
        acc = acc + home[e, :hidden_rows, :].astype(F32)
    turned = acc.T
    for t in range(3):
        shared[t] = acc[t * cols : (t + 1) * cols]
    row = jnp.sum(turned * turned, axis=0, keepdims=True)
    fill = lines.shape[1] * width - quarter.shape[0] * width - hidden_rows
    row = jnp.concatenate([row, jnp.zeros((1, fill), F32)], 1)
    parts = [quarter[...]] + [row[:, a : a + width] for a in range(0, row.shape[1], width)]
    lines[...] = jnp.broadcast_to(jnp.concatenate(parts, 0).astype(BF)[None], lines.shape)


def finish_norms(scale, pos, lines, other, e_norm, s_norm):
    n, block, width = lines.shape
    _, le, hidden = e_norm.shape
    cols = s_norm.shape[1]
    q = 3 * le * hidden // (4 * width)
    c = pos[1]
    sums = []
    for ref in (lines, other):
        for b in range(2):
            acc = ref[b].astype(F32)
            for d in range(2 + b, n, 2):
                acc = acc + ref[d].astype(F32)
            sums.append(acc)
    rows = [jnp.where(c == 0, sums[k], sums[(k + 2) % 4]) for k in range(4)]
    whole = rows[0] + rows[1] + rows[2] + rows[3]
    rows = [r[i : i + 1] * scale for r in rows for i in range(q)]
    per = hidden // width
    for t in range(3):
        for e in range(le):
            at = (t * le + e) * per
            e_norm[t, e : e + 1, :] = jnp.concatenate(rows[at : at + per], 1)
    line = jnp.concatenate([whole[i : i + 1] for i in range(q, block)], 1) * scale
    for t in range(3):
        s_norm[t : t + 1, :] = line[:, t * cols : (t + 1) * cols]


def project(sizes, pos, got, both, *refs):
    weights, results = refs[:6], refs[6:10]
    xt_ref, gt_ref, xs_ref, gs_ref = refs[10:14]
    held, made = refs[14:17], refs[17:21]
    sem_in, sem_out = refs[21], refs[22]
    le, width, hidden = weights[0].shape
    loads = []
    for t in range(3):
        for e in range(le + 1):
            src = weights[t].at[e] if e < le else weights[3 + t]
            to = held[t].at[e * width : (e + 1) * width, :]
            loads.append(pltpu.make_async_copy(src, to, sem_in.at[t, e]))
            loads[-1].start()
    nb, rows = got.shape[0], both.shape[0]
    sec = made[0].shape[0]
    half = 2 * sec
    z, c = pos[0], pos[1]
    src, kd, _, _ = ring_rows(along(2 * half, 0), z, c, sizes)
    cols = lax.broadcasted_iota(jnp.int32, (2 * half, nb), 1)
    mine = mm(one_hot(src, cols), got[...])
    mine = mine + mm(one_hot(src - nb, lax.broadcasted_iota(jnp.int32, (2 * half, rows), 1)), both[...])
    part = [jnp.where(kd == e, mine, 0.0).astype(BF) for e in range(le + 1)]
    x = jnp.concatenate([p[:, :width] for p in part], 1)
    g = jnp.concatenate([p[:, width:] for p in part], 1)
    stores = []
    for t, lhs in enumerate((x, x, g)):
        cut = slice(t * hidden, (t + 1) * hidden)
        for load in loads[t * (le + 1) : (t + 1) * (le + 1)]:
            load.wait()
        p = mm(lhs, held[t][...])
        for k in (3, 1, 2, 0):
            at = (0, sec, half, half + sec)[k]
            made[k][:, cut] = p[at : at + sec].astype(made[k].dtype)
            store = pltpu.make_async_copy(made[k].at[:, cut], results[k].at[:, cut], sem_out.at[t, k])
            store.start()
            stores.append(store)
    _, kr, _, _ = ring_rows(along(2 * half, 1), z, c, sizes)
    mine_t = mine.T
    for e in range(le + 1):
        both_t = jnp.where(kr == e, mine_t, 0.0).astype(BF)
        to_x, to_g, at = (xt_ref, gt_ref, e * width) if e < le else (xs_ref, gs_ref, 0)
        to_x[at : at + width, :] = both_t[:width]
        to_g[at : at + width, :] = both_t[width:]
    for store in stores:
        store.wait()


def over_rows(lhs, parts, cut):
    at, out = 0, None
    for p in parts:
        n = p.shape[0]
        r = mm(lhs[:, at : at + n], p[:, cut])
        out = r if out is None else out + r
        at += n
    return out


def stack_rows(*refs):
    at, out = 0, refs[-1]
    for ref in refs[:-1]:
        out[at : at + ref.shape[0], :] = ref[...]
        at += ref.shape[0]


def expert_grads(g0, g1, g2, g3, xt, gt, after, stack, sq):
    _, le, width, hidden = stack.shape
    for t, lhs in enumerate((xt, xt, gt)):
        r = over_rows(lhs, (g0, g1, g2, g3), slice(t * hidden, (t + 1) * hidden)).reshape(le, width, hidden)
        stack[t] = r.astype(BF)
        total = jnp.sum(r * r, axis=1, keepdims=True)
        per = hidden // width
        for e in range(le):
            for q in range(per):
                at = (t * le + e) * per + q
                sq[at : at + 1, :] = total[e, :, q * width : (q + 1) * width]


def row_grads(sizes, pos, g0, g1, g2, g3, eg, eu, sg, su, xs, gs, out, shared):
    le, width, hidden = eg.shape
    ls, bl = sizes[2], sizes[4]
    n_ep, rows = out.shape[0], shared.shape[0]
    nb = n_ep * bl
    cols = hidden // n_ep
    for t, lhs in enumerate((xs, xs, gs)):
        r = over_rows(lhs, (g0, g1, g2, g3), slice(t * hidden, (t + 1) * hidden))
        out[:, t * cols : (t + 1) * cols, :] = r.T.astype(BF).reshape(n_ep, cols, width)
    total = 2 * sizes[0] * sizes[1]
    z, c = pos[0], pos[1]
    _, kd, _, within = ring_rows(along(total, 0), z, c, sizes)
    slots, wg, at = [], [], 0
    for src in (g0, g1, g2, g3):
        n = src.shape[0]
        gg, gu = src[:, :hidden], src[:, hidden : 2 * hidden]
        se = mm(gg, eg[...].reshape(le * width, hidden), NT) + mm(gu, eu[...].reshape(le * width, hidden), NT)
        ss = mm(gg, sg[...], NT) + mm(gu, su[...], NT)
        k = kd[at : at + n]
        s = jnp.where(k == le, ss, 0.0)
        for e in range(le):
            s = s + jnp.where(k == e, se[:, e * width : (e + 1) * width], 0.0)
        slots.append(s)
        lanes = lax.broadcasted_iota(jnp.int32, (n, width), 1)
        wg.append(jnp.where(within[at : at + n] == lanes, src[:, 3 * hidden :].astype(F32), 0.0))
        at += n
    slot = jnp.concatenate(slots, 0)
    hi = slot.astype(BF)
    rest = slot - hi.astype(F32)
    mid = rest.astype(BF)
    low = (rest - mid.astype(F32)).astype(BF)
    src_r, _, block, _ = ring_rows(along(total, 1), z, c, sizes)
    lines = lax.broadcasted_iota(jnp.int32, (nb, total), 0)
    to_slot = one_hot(lines, src_r)
    to_tail = one_hot(lines, jnp.where(block >= 0, block * bl + ls, -1))
    back = mm(to_slot, hi) + mm(to_tail, jnp.concatenate(wg, 0).astype(BF))
    out[:, 3 * cols :, :] = back.reshape(n_ep, bl, width).astype(BF)
    ps = one_hot(lax.broadcasted_iota(jnp.int32, (rows, total), 0) + nb, src_r)
    shared[...] = mm(ps, hi) + mm(ps, mid) + mm(ps, low)


def row_backward(summed, weights):
    hidden = summed.shape[1] // 3
    pre_gate = summed[:, :hidden]
    pre_up = summed[:, hidden : 2 * hidden]
    back_act = summed[:, 2 * hidden :]
    sigmoid_gate = jax.nn.sigmoid(pre_gate)
    silu_gate = pre_gate * sigmoid_gate
    activation = silu_gate * pre_up
    act_grad = weights * back_act
    grad_up = (act_grad * silu_gate).astype(BF)
    grad_gate = (act_grad * pre_up * sigmoid_gate * (1.0 + pre_gate * (1.0 - sigmoid_gate))).astype(BF)
    scaled_act = (weights * activation).astype(BF)
    weight_grad = jnp.sum(activation * back_act, axis=1, keepdims=True).astype(BF)
    return grad_gate, grad_up, scaled_act, weight_grad


def body(tokens, cotangent, routes, gate_weights, e_gate, e_up, e_down, s_gate, s_up, s_down):
    n_ep, n_tp = lax.axis_size("ep"), lax.axis_size("tp")
    nz = n_tp // 2
    rows, width = tokens.shape
    top = routes.shape[1]
    le, _, hidden = e_gate.shape
    experts = le * n_ep
    cap = 3 * rows * top // (2 * experts)
    ls = le * cap
    bl = (ls + 8) // 8 * 8
    slots = n_ep * ls
    total = slots + rows
    piece = total // n_tp
    tp = lax.axis_index("tp")
    z, c = tp // 2, tp % 2
    fwd = [(i, (i + 4 - 8 * (i % 2)) % n_tp) for i in range(n_tp)]
    bwd = [(b, a) for a, b in fwd]
    pair = [(i, (2 * ((i // 2 + i % 2) % nz ^ 1) - i % 2) % n_tp) for i in range(n_tp)]
    swap = [(i, i ^ 1) for i in range(n_tp)]

    geo = (le, cap, experts, bl)
    lanes = jnp.arange(2 * width, dtype=jnp.int32)
    groups = jnp.arange(n_ep, dtype=jnp.int32)
    sent, both = call(
        functools.partial(dispatch, geo),
        [((n_ep * bl, 2 * width), BF), ((rows, 2 * width), BF)],
        tokens, cotangent, routes.T, gate_weights.T,
    )
    got = lax.all_to_all(sent.reshape(n_ep, bl, 2 * width), "ep", 0, 0, tiled=True)

    sizes = (nz, piece, ls, cap, bl, slots)
    pos = jnp.stack([z, c]).astype(jnp.int32)
    members = nz // 2
    hops, back_hops = members // 2, members - members // 2 - 1
    sec = members * piece
    width3 = 3 * hidden
    big = [((sec, width3), F32)] * 2 + [((sec, width3), BF)] * 2
    turned = [((le * width, total), BF)] * 2 + [((width, total), BF)] * 2
    weights = (e_gate, e_up, e_down, s_gate, s_up, s_down)
    anywhere = pl.BlockSpec(memory_space=pl.ANY)
    own_k, own_s, out_k, out_s, xt, gt, xs, gs = pl.pallas_call(
        functools.partial(project, sizes),
        out_shape=[jax.ShapeDtypeStruct(a, d) for a, d in big + turned],
        in_specs=[pl.BlockSpec(memory_space=pltpu.SMEM), VM, VM] + [anywhere] * 6,
        out_specs=[anywhere] * 4 + [VM] * 4,
        scratch_shapes=[pltpu.VMEM(((le + 1) * width, hidden), BF)] * 3
        + [pltpu.VMEM(a, d) for a, d in big]
        + [pltpu.SemaphoreType.DMA((3, le + 1)), pltpu.SemaphoreType.DMA((3, 4))],
    )(pos, got.reshape(n_ep * bl, 2 * width), both, *weights)
    oth_s = lax.ppermute(out_s, "tp", swap)
    oth_k = lax.ppermute(out_k, "tp", swap)
    cut = 2 * piece
    to_a = (own_s[:cut] + oth_s[:cut].astype(F32)).astype(BF)
    to_b = (own_s[cut:] + oth_s[cut:].astype(F32)).astype(BF)
    par_a = lax.ppermute(to_a, "tp", pair)
    par_b = lax.ppermute(to_b, "tp", pair)
    left_rows = slice(cut, hops * piece)
    on_left = lax.optimization_barrier((own_k[left_rows], oth_k[left_rows], par_b[: hops * piece - cut]))

    def at(m):
        p = (m - hops) % members
        rows_p = slice(p * piece, (p + 1) * piece)
        par = par_a[rows_p] if p < 2 else par_b[p * piece - cut : (p + 1) * piece - cut]
        own, oth = own_k, oth_k
        if 1 < p < hops:
            (own, oth, par), rows_p = on_left, slice((p - 2) * piece, (p - 1) * piece)
            par = par[rows_p]
        return own[rows_p] + oth[rows_p].astype(F32) + par.astype(F32)

    right, left = at(hops).astype(BF), at(hops + 1).astype(BF)
    for t in range(hops):
        right = lax.ppermute(right, "tp", fwd)
        if t < hops - 1:
            right = (right.astype(F32) + at(hops - 1 - t)).astype(BF)
        if t < back_hops:
            left = lax.ppermute(left, "tp", bwd)
        if t < back_hops - 1:
            left = (left.astype(F32) + at(hops + 2 + t)).astype(BF)
    summed = right.astype(F32) + left.astype(F32) + at(0)

    q = tp * piece + jnp.arange(piece, dtype=jnp.int32)
    w_rows = mm(hot((q // ls)[:, None], groups[None, :]), got[:, ls, :])
    own_w = jnp.sum(jnp.where((q % ls)[:, None] == lanes[None, :], w_rows, 0.0), axis=1)
    own_w = jnp.where(q < slots, own_w, 1.0)[:, None]
    gg, gu, sa, wg = row_backward(summed, own_w)
    block = jnp.concatenate([gg, gu, sa, jnp.broadcast_to(wg, (piece, 128))], 1)

    ring = [None] * members
    ring[0] = right = left = block
    for t in range(1, hops + 1):
        right = lax.ppermute(right, "tp", fwd)
        ring[-t % members] = right
        if t <= back_hops:
            left = lax.ppermute(left, "tp", bwd)
            ring[t] = left
    parts = ring[hops + 1 :] + ring[:hops]
    (most,) = call(stack_rows, [((len(parts) * piece, block.shape[1]), BF)], *parts, limit=8 * 2**20)
    most_o = lax.ppermute(most, "tp", pair)
    last_o = lax.ppermute(ring[hops], "tp", pair)
    kept = jnp.concatenate([ring[hops], most], 0)
    kept_x = lax.ppermute(kept, "tp", swap)
    paired = jnp.concatenate([last_o, most_o], 0)
    paired_x = lax.ppermute(paired, "tp", swap)
    grads = (kept, paired, kept_x, paired_x)

    cols = hidden // n_ep
    out, shared_part = call(
        functools.partial(row_grads, sizes),
        [((n_ep, 3 * cols + bl, width), BF), ((rows, width), F32)],
        pos, *grads, e_gate, e_up, s_gate, s_up, xs, gs, smem=1,
    )
    home = lax.all_to_all(out, "ep", 0, 0, tiled=True)
    stack, e_sq = call(
        expert_grads, [((3, le, width, hidden), BF), ((3 * le * hidden // width, width), F32)], *grads, xt, gt, out, rest=1
    )
    e_sq = e_sq.reshape(2, -1, width)
    other_sq = lax.ppermute(jnp.where(c == 0, e_sq[1], e_sq[0]), "tp", swap)
    e_sq = (jnp.where(c == 0, e_sq[0], e_sq[1]) + other_sq).reshape(2, -1, width)
    other_sq = lax.ppermute(jnp.where(z % 2 == 0, e_sq[1], e_sq[0]), "tp", [(i, i ^ 2) for i in range(n_tp)])
    e_sq = jnp.where(z % 2 == 0, e_sq[0], e_sq[1]) + other_sq
    n_lines = (e_sq.shape[0] + -(-3 * cols // width) + 15) // 16 * 16
    shared, lines = call(
        gather_norms, [((3, cols, width), F32), ((nz, n_lines, width), BF)], home, e_sq
    )
    same_core = [[2 * i + k for i in range(nz)] for k in range(2)]
    got_lines = lax.all_to_all(lines, "tp", 0, 0, axis_index_groups=same_core, tiled=True)
    token_grad, gate_grad = call(
        functools.partial(collect, geo),
        [((rows, width), BF), ((top, rows), F32)],
        home, shared_part, routes.T, lines, rest=1,
    )
    other_lines = lax.ppermute(got_lines, "tp", swap)
    e_norm, s_norm = call(
        functools.partial(finish_norms, 1.0 / (width * n_tp)),
        [((3, le, hidden), F32), ((3, cols), F32)],
        pos, got_lines, other_lines, smem=1,
    )
    return token_grad, gate_grad.astype(BF).T, stack, jnp.swapaxes(shared, 1, 2), e_norm, s_norm


def solution(mesh):
    return jax.shard_map(
        body,
        mesh=mesh,
        in_specs=(
            P("ep", "tp"),
            P("ep", "tp"),
            P("ep", None),
            P("ep", None),
            P("ep", "tp", None),
            P("ep", "tp", None),
            P("ep", "tp", None),
            P("tp", None),
            P("tp", None),
            P("tp", None),
        ),
        out_specs=(
            P("ep", "tp"),
            P("ep", None),
            P(None, "ep", "tp", None),
            P(None, "tp", "ep"),
            P(None, "ep", None),
            P(None, "ep"),
        ),
        check_vma=False,
    )
```

```python
import functools

import jax
import jax.numpy as jnp
from jax import lax
from jax.experimental import pallas as pl
from jax.experimental.pallas import tpu as pltpu
from jax.sharding import PartitionSpec as P


BF = jnp.bfloat16
F32 = jnp.float32
VM = pl.BlockSpec(memory_space=pltpu.VMEM)


def mm(a, b, dims=((1,), (0,))):
    return lax.dot_general(a, b, (dims, ((), ())), preferred_element_type=F32)


NT = ((1,), (1,))


def hot(a, b):
    return (a == b).astype(BF)


def call(kernel, outs, *args, smem=0, rest=0, limit=None):
    first = [pl.BlockSpec(memory_space=pltpu.SMEM)] * smem
    last = [pl.BlockSpec(memory_space=pl.ANY)] * rest
    return pl.pallas_call(
        kernel,
        out_shape=[jax.ShapeDtypeStruct(s, d) for s, d in outs],
        in_specs=first + [VM] * (len(args) - smem - rest) + last,
        out_specs=[VM] * len(outs),
        compiler_params=pltpu.CompilerParams(vmem_limit_bytes=limit),
    )(*args)


def quotient(n, by, top):
    shift = 0
    while (1 << shift) < by * top:
        shift += 1
    factor = -(-(1 << shift) // by)
    assert factor * top < 2**31
    return lax.shift_right_logical(n * factor, jnp.int32(shift))


def ring_rows(r, z, c, sizes):
    nz, piece, ls, cap, bl, slots = sizes
    sec = nz // 2 * piece
    half = 2 * sec
    h = (r >= half).astype(jnp.int32)
    inner = r - half * h
    q = (inner >= sec).astype(jnp.int32)
    inner = inner - sec * q
    m = quotient(inner, piece, sec)
    core = jnp.abs(c - h)
    zeta = (z + core) & (nz - 1)
    zeta = zeta + q * (1 - 2 * (zeta & 1)) + 2 * (1 - 2 * core) * (m + nz // 4)
    place = piece * (2 * ((zeta - core) & (nz - 1)) + core) + inner - piece * m
    block = quotient(place, ls, 2 * half)
    within = place - ls * block
    routed = place < slots
    expert = jnp.where(routed, quotient(within, cap, ls), ls // cap)
    src = jnp.where(routed, block * bl + within, slots // ls * bl + place - slots)
    return src, expert, jnp.where(routed, block, -1), within


def along(n, dim):
    return lax.broadcasted_iota(jnp.int32, (n, 1) if dim == 0 else (1, n), dim)


def one_hot(a, b):
    return jnp.where(a == b, 1.0, 0.0).astype(BF)


def columns(lines):
    lines = lines.astype(F32)
    return jnp.concatenate([lines, jnp.zeros((8 - lines.shape[0], lines.shape[1]), F32)], 0).T


def routing(routes, le, cap, experts):
    top, rows = routes.shape
    routes = columns(routes).astype(jnp.int32)
    lanes = lax.broadcasted_iota(jnp.int32, (rows, experts), 1)
    chosen = [routes[:, k : k + 1] for k in range(top)]
    on = [jnp.where(f == lanes, 1.0, 0.0) for f in chosen]
    shape = (rows, rows)
    tri = jnp.where(lax.broadcasted_iota(jnp.int32, shape, 0) > lax.broadcasted_iota(jnp.int32, shape, 1), 1.0, 0.0)
    before = mm(tri.astype(BF), sum(on).astype(BF))
    out = []
    for f, o in zip(chosen, on):
        dest = quotient(f, le, experts)
        pos = jnp.sum(o * before, axis=1, keepdims=True).astype(jnp.int32)
        out.append((dest, (f - le * dest) * cap + pos))
    return out


def dispatch(geo, tokens, cotangent, routes, weights, sent, both):
    le, cap, experts, bl = geo
    rows, width = tokens.shape
    n = sent.shape[0]
    xg = jnp.concatenate([tokens[...], cotangent[...]], 1)
    both[...] = xg
    where = routing(routes[...], le, cap, experts)
    cols = lax.broadcasted_iota(jnp.int32, (rows, n), 1)
    lanes = lax.broadcasted_iota(jnp.int32, (rows, 2 * width), 1)
    w = columns(weights[...])
    left, right = [jnp.zeros((rows, n), F32)], [xg]
    for k, (dest, within) in enumerate(where):
        left[0] = left[0] + jnp.where(dest * bl + within == cols, 1.0, 0.0)
        left.append(jnp.where(dest * bl + le * cap == cols, w[:, k : k + 1], 0.0))
        right.append(one_hot(within, lanes))
    left = jnp.concatenate([a.T.astype(BF) for a in left], 1)
    sent[...] = mm(left, jnp.concatenate(right, 0)).astype(BF)


def collect(geo, home, shared, routes, after, token_grad, gate_grad):
    le, cap, experts, bl = geo
    n_ep = home.shape[0]
    rows, width = shared.shape
    n = n_ep * bl
    first = home.shape[1] - bl
    where = routing(routes[...], le, cap, experts)
    cols = lax.broadcasted_iota(jnp.int32, (rows, n), 1)
    lanes = lax.broadcasted_iota(jnp.int32, (rows, width), 1)
    back = home[:, first:, :].astype(F32).reshape(n, width).astype(BF)
    pick, picked = jnp.zeros((rows, n), F32), []
    for dest, within in where:
        pick = pick + jnp.where(dest * bl + within == cols, 1.0, 0.0)
        line = mm(one_hot(dest * bl + le * cap, cols), back)
        picked.append(jnp.sum(jnp.where(within == lanes, line, 0.0), axis=1, keepdims=True))
    picked.append(jnp.zeros((rows, 8 - len(picked)), F32))
    gate_grad[...] = jnp.concatenate(picked, 1).T[: gate_grad.shape[0]]
    token_grad[...] = (mm(pick.astype(BF), back) + shared[...]).astype(BF)


def gather_norms(home, quarter, shared, lines):
    _, cols, width = shared.shape
    hidden_rows = 3 * cols
    acc = home[0, :hidden_rows, :].astype(F32)
    for e in range(1, home.shape[0]):
        acc = acc + home[e, :hidden_rows, :].astype(F32)
    turned = acc.T
    for t in range(3):
        shared[t] = acc[t * cols : (t + 1) * cols]
    row = jnp.sum(turned * turned, axis=0, keepdims=True)
    fill = lines.shape[1] * width - quarter.shape[0] * width - hidden_rows
    row = jnp.concatenate([row, jnp.zeros((1, fill), F32)], 1)
    parts = [quarter[...]] + [row[:, a : a + width] for a in range(0, row.shape[1], width)]
    lines[...] = jnp.broadcast_to(jnp.concatenate(parts, 0).astype(BF)[None], lines.shape)


def finish_norms(scale, pos, lines, other, e_norm, s_norm):
    n, block, width = lines.shape
    _, le, hidden = e_norm.shape
    cols = s_norm.shape[1]
    q = 3 * le * hidden // (4 * width)
    c = pos[1]
    sums = []
    for ref in (lines, other):
        for b in range(2):
            acc = ref[b].astype(F32)
            for d in range(2 + b, n, 2):
                acc = acc + ref[d].astype(F32)
            sums.append(acc)
    rows = [jnp.where(c == 0, sums[k], sums[(k + 2) % 4]) for k in range(4)]
    whole = rows[0] + rows[1] + rows[2] + rows[3]
    rows = [r[i : i + 1] * scale for r in rows for i in range(q)]
    per = hidden // width
    for t in range(3):
        for e in range(le):
            at = (t * le + e) * per
            e_norm[t, e : e + 1, :] = jnp.concatenate(rows[at : at + per], 1)
    line = jnp.concatenate([whole[i : i + 1] for i in range(q, block)], 1) * scale
    for t in range(3):
        s_norm[t : t + 1, :] = line[:, t * cols : (t + 1) * cols]


def project(sizes, pos, got, both, *refs):
    weights, results = refs[:6], refs[6:10]
    xt_ref, gt_ref, xs_ref, gs_ref = refs[10:14]
    held, made = refs[14:17], refs[17:21]
    sem_in, sem_out = refs[21], refs[22]
    le, width, hidden = weights[0].shape
    loads = []
    for t in range(3):
        for e in range(le + 1):
            src = weights[t].at[e] if e < le else weights[3 + t]
            to = held[t].at[e * width : (e + 1) * width, :]
            loads.append(pltpu.make_async_copy(src, to, sem_in.at[t, e]))
            loads[-1].start()
    nb, rows = got.shape[0], both.shape[0]
    sec = made[0].shape[0]
    half = 2 * sec
    z, c = pos[0], pos[1]
    src, kd, _, _ = ring_rows(along(2 * half, 0), z, c, sizes)
    cols = lax.broadcasted_iota(jnp.int32, (2 * half, nb), 1)
    mine = mm(one_hot(src, cols), got[...])
    mine = mine + mm(one_hot(src - nb, lax.broadcasted_iota(jnp.int32, (2 * half, rows), 1)), both[...])
    part = [jnp.where(kd == e, mine, 0.0).astype(BF) for e in range(le + 1)]
    x = jnp.concatenate([p[:, :width] for p in part], 1)
    g = jnp.concatenate([p[:, width:] for p in part], 1)
    stores = []
    for t, lhs in enumerate((x, x, g)):
        cut = slice(t * hidden, (t + 1) * hidden)
        for load in loads[t * (le + 1) : (t + 1) * (le + 1)]:
            load.wait()
        p = mm(lhs, held[t][...])
        for k in (3, 1, 2, 0):
            at = (0, sec, half, half + sec)[k]
            made[k][:, cut] = p[at : at + sec].astype(made[k].dtype)
            store = pltpu.make_async_copy(made[k].at[:, cut], results[k].at[:, cut], sem_out.at[t, k])
            store.start()
            stores.append(store)
    _, kr, _, _ = ring_rows(along(2 * half, 1), z, c, sizes)
    mine_t = mine.T
    for e in range(le + 1):
        both_t = jnp.where(kr == e, mine_t, 0.0).astype(BF)
        to_x, to_g, at = (xt_ref, gt_ref, e * width) if e < le else (xs_ref, gs_ref, 0)
        to_x[at : at + width, :] = both_t[:width]
        to_g[at : at + width, :] = both_t[width:]
    for store in stores:
        store.wait()


def over_rows(lhs, parts, cut):
    at, out = 0, None
    for p in parts:
        n = p.shape[0]
        r = mm(lhs[:, at : at + n], p[:, cut])
        out = r if out is None else out + r
        at += n
    return out


def stack_rows(*refs):
    at, out = 0, refs[-1]
    for ref in refs[:-1]:
        out[at : at + ref.shape[0], :] = ref[...]
        at += ref.shape[0]


def expert_grads(g0, g1, g2, g3, xt, gt, after, stack, sq):
    _, le, width, hidden = stack.shape
    for t, lhs in enumerate((xt, xt, gt)):
        r = over_rows(lhs, (g0, g1, g2, g3), slice(t * hidden, (t + 1) * hidden)).reshape(le, width, hidden)
        stack[t] = r.astype(BF)
        total = jnp.sum(r * r, axis=1, keepdims=True)
        per = hidden // width
        for e in range(le):
            for q in range(per):
                at = (t * le + e) * per + q
                sq[at : at + 1, :] = total[e, :, q * width : (q + 1) * width]


def row_grads(sizes, pos, g0, g1, g2, g3, eg, eu, sg, su, xs, gs, out, shared):
    le, width, hidden = eg.shape
    ls, bl = sizes[2], sizes[4]
    n_ep, rows = out.shape[0], shared.shape[0]
    nb = n_ep * bl
    cols = hidden // n_ep
    for t, lhs in enumerate((xs, xs, gs)):
        r = over_rows(lhs, (g0, g1, g2, g3), slice(t * hidden, (t + 1) * hidden))
        out[:, t * cols : (t + 1) * cols, :] = r.T.astype(BF).reshape(n_ep, cols, width)
    total = 2 * sizes[0] * sizes[1]
    z, c = pos[0], pos[1]
    _, kd, _, within = ring_rows(along(total, 0), z, c, sizes)
    slots, wg, at = [], [], 0
    for src in (g0, g1, g2, g3):
        n = src.shape[0]
        gg, gu = src[:, :hidden], src[:, hidden : 2 * hidden]
        se = mm(gg, eg[...].reshape(le * width, hidden), NT) + mm(gu, eu[...].reshape(le * width, hidden), NT)
        ss = mm(gg, sg[...], NT) + mm(gu, su[...], NT)
        k = kd[at : at + n]
        s = jnp.where(k == le, ss, 0.0)
        for e in range(le):
            s = s + jnp.where(k == e, se[:, e * width : (e + 1) * width], 0.0)
        slots.append(s)
        lanes = lax.broadcasted_iota(jnp.int32, (n, width), 1)
        wg.append(jnp.where(within[at : at + n] == lanes, src[:, 3 * hidden :].astype(F32), 0.0))
        at += n
    slot = jnp.concatenate(slots, 0)
    hi = slot.astype(BF)
    rest = slot - hi.astype(F32)
    mid = rest.astype(BF)
    low = (rest - mid.astype(F32)).astype(BF)
    src_r, _, block, _ = ring_rows(along(total, 1), z, c, sizes)
    lines = lax.broadcasted_iota(jnp.int32, (nb, total), 0)
    to_slot = one_hot(lines, src_r)
    to_tail = one_hot(lines, jnp.where(block >= 0, block * bl + ls, -1))
    back = mm(to_slot, hi) + mm(to_tail, jnp.concatenate(wg, 0).astype(BF))
    out[:, 3 * cols :, :] = back.reshape(n_ep, bl, width).astype(BF)
    ps = one_hot(lax.broadcasted_iota(jnp.int32, (rows, total), 0) + nb, src_r)
    shared[...] = mm(ps, hi) + mm(ps, mid) + mm(ps, low)


def row_backward(summed, weights):
    hidden = summed.shape[1] // 3
    pre_gate = summed[:, :hidden]
    pre_up = summed[:, hidden : 2 * hidden]
    back_act = summed[:, 2 * hidden :]
    sigmoid_gate = jax.nn.sigmoid(pre_gate)
    silu_gate = pre_gate * sigmoid_gate
    activation = silu_gate * pre_up
    act_grad = weights * back_act
    grad_up = (act_grad * silu_gate).astype(BF)
    grad_gate = (act_grad * pre_up * sigmoid_gate * (1.0 + pre_gate * (1.0 - sigmoid_gate))).astype(BF)
    scaled_act = (weights * activation).astype(BF)
    weight_grad = jnp.sum(activation * back_act, axis=1, keepdims=True).astype(BF)
    return grad_gate, grad_up, scaled_act, weight_grad


def body(tokens, cotangent, routes, gate_weights, e_gate, e_up, e_down, s_gate, s_up, s_down):
    n_ep, n_tp = lax.axis_size("ep"), lax.axis_size("tp")
    nz = n_tp // 2
    rows, width = tokens.shape
    top = routes.shape[1]
    le, _, hidden = e_gate.shape
    experts = le * n_ep
    cap = 3 * rows * top // (2 * experts)
    ls = le * cap
    bl = (ls + 8) // 8 * 8
    slots = n_ep * ls
    total = slots + rows
    piece = total // n_tp
    tp = lax.axis_index("tp")
    z, c = tp // 2, tp % 2
    fwd = [(i, (i + 4 - 8 * (i % 2)) % n_tp) for i in range(n_tp)]
    bwd = [(b, a) for a, b in fwd]
    pair = [(i, (2 * ((i // 2 + i % 2) % nz ^ 1) - i % 2) % n_tp) for i in range(n_tp)]
    swap = [(i, i ^ 1) for i in range(n_tp)]

    geo = (le, cap, experts, bl)
    lanes = jnp.arange(2 * width, dtype=jnp.int32)
    groups = jnp.arange(n_ep, dtype=jnp.int32)
    sent, both = call(
        functools.partial(dispatch, geo),
        [((n_ep * bl, 2 * width), BF), ((rows, 2 * width), BF)],
        tokens, cotangent, routes.T, gate_weights.T,
    )
    got = lax.all_to_all(sent.reshape(n_ep, bl, 2 * width), "ep", 0, 0, tiled=True)

    sizes = (nz, piece, ls, cap, bl, slots)
    pos = jnp.stack([z, c]).astype(jnp.int32)
    members = nz // 2
    hops, back_hops = members // 2, members - members // 2 - 1
    sec = members * piece
    width3 = 3 * hidden
    big = [((sec, width3), F32)] * 2 + [((sec, width3), BF)] * 2
    turned = [((le * width, total), BF)] * 2 + [((width, total), BF)] * 2
    weights = (e_gate, e_up, e_down, s_gate, s_up, s_down)
    anywhere = pl.BlockSpec(memory_space=pl.ANY)
    own_k, own_s, out_k, out_s, xt, gt, xs, gs = pl.pallas_call(
        functools.partial(project, sizes),
        out_shape=[jax.ShapeDtypeStruct(a, d) for a, d in big + turned],
        in_specs=[pl.BlockSpec(memory_space=pltpu.SMEM), VM, VM] + [anywhere] * 6,
        out_specs=[anywhere] * 4 + [VM] * 4,
        scratch_shapes=[pltpu.VMEM(((le + 1) * width, hidden), BF)] * 3
        + [pltpu.VMEM(a, d) for a, d in big]
        + [pltpu.SemaphoreType.DMA((3, le + 1)), pltpu.SemaphoreType.DMA((3, 4))],
    )(pos, got.reshape(n_ep * bl, 2 * width), both, *weights)
    oth_s = lax.ppermute(out_s, "tp", swap)
    oth_k = lax.ppermute(out_k, "tp", swap)
    cut = 2 * piece
    to_a = (own_s[:cut] + oth_s[:cut].astype(F32)).astype(BF)
    to_b = (own_s[cut:] + oth_s[cut:].astype(F32)).astype(BF)
    par_a = lax.ppermute(to_a, "tp", pair)
    par_b = lax.ppermute(to_b, "tp", pair)
    left_rows = slice(cut, hops * piece)
    on_left = lax.optimization_barrier((own_k[left_rows], oth_k[left_rows], par_b[: hops * piece - cut]))

    def at(m):
        p = (m - hops) % members
        rows_p = slice(p * piece, (p + 1) * piece)
        par = par_a[rows_p] if p < 2 else par_b[p * piece - cut : (p + 1) * piece - cut]
        own, oth = own_k, oth_k
        if 1 < p < hops:
            (own, oth, par), rows_p = on_left, slice((p - 2) * piece, (p - 1) * piece)
            par = par[rows_p]
        return own[rows_p] + oth[rows_p].astype(F32) + par.astype(F32)

    right, left = at(hops).astype(BF), at(hops + 1).astype(BF)
    for t in range(hops):
        right = lax.ppermute(right, "tp", fwd)
        if t < hops - 1:
            right = (right.astype(F32) + at(hops - 1 - t)).astype(BF)
        if t < back_hops:
            left = lax.ppermute(left, "tp", bwd)
        if t < back_hops - 1:
            left = (left.astype(F32) + at(hops + 2 + t)).astype(BF)
    summed = right.astype(F32) + left.astype(F32) + at(0)

    q = tp * piece + jnp.arange(piece, dtype=jnp.int32)
    w_rows = mm(hot((q // ls)[:, None], groups[None, :]), got[:, ls, :])
    own_w = jnp.sum(jnp.where((q % ls)[:, None] == lanes[None, :], w_rows, 0.0), axis=1)
    own_w = jnp.where(q < slots, own_w, 1.0)[:, None]
    gg, gu, sa, wg = row_backward(summed, own_w)
    block = jnp.concatenate([gg, gu, sa, jnp.broadcast_to(wg, (piece, 128))], 1)

    ring = [None] * members
    ring[0] = right = left = block
    for t in range(1, hops + 1):
        right = lax.ppermute(right, "tp", fwd)
        ring[-t % members] = right
        if t <= back_hops:
            left = lax.ppermute(left, "tp", bwd)
            ring[t] = left
    parts = ring[hops + 1 :] + ring[: hops - 1]
    (most,) = call(stack_rows, [((len(parts) * piece, block.shape[1]), BF)], *parts, limit=8 * 2**20)
    most_o = lax.ppermute(most, "tp", pair)
    left_o = lax.ppermute(ring[hops - 1], "tp", pair)
    last_o = lax.ppermute(ring[hops], "tp", pair)
    kept = jnp.concatenate([ring[hops], most, ring[hops - 1]], 0)
    kept_x = lax.ppermute(kept, "tp", swap)
    paired = jnp.concatenate([last_o, most_o, left_o], 0)
    paired_x = lax.ppermute(paired, "tp", swap)
    grads = (kept, paired, kept_x, paired_x)

    cols = hidden // n_ep
    out, shared_part = call(
        functools.partial(row_grads, sizes),
        [((n_ep, 3 * cols + bl, width), BF), ((rows, width), F32)],
        pos, *grads, e_gate, e_up, s_gate, s_up, xs, gs, smem=1,
    )
    home = lax.all_to_all(out, "ep", 0, 0, tiled=True)
    stack, e_sq = call(
        expert_grads, [((3, le, width, hidden), BF), ((3 * le * hidden // width, width), F32)], *grads, xt, gt, out, rest=1
    )
    e_sq = e_sq.reshape(2, -1, width)
    other_sq = lax.ppermute(jnp.where(c == 0, e_sq[1], e_sq[0]), "tp", swap)
    e_sq = (jnp.where(c == 0, e_sq[0], e_sq[1]) + other_sq).reshape(2, -1, width)
    other_sq = lax.ppermute(jnp.where(z % 2 == 0, e_sq[1], e_sq[0]), "tp", [(i, i ^ 2) for i in range(n_tp)])
    e_sq = jnp.where(z % 2 == 0, e_sq[0], e_sq[1]) + other_sq
    n_lines = (e_sq.shape[0] + -(-3 * cols // width) + 15) // 16 * 16
    shared, lines = call(
        gather_norms, [((3, cols, width), F32), ((nz, n_lines, width), BF)], home, e_sq
    )
    same_core = [[2 * i + k for i in range(nz)] for k in range(2)]
    got_lines = lax.all_to_all(lines, "tp", 0, 0, axis_index_groups=same_core, tiled=True)
    token_grad, gate_grad = call(
        functools.partial(collect, geo),
        [((rows, width), BF), ((top, rows), F32)],
        home, shared_part, routes.T, lines, rest=1,
    )
    other_lines = lax.ppermute(got_lines, "tp", swap)
    e_norm, s_norm = call(
        functools.partial(finish_norms, 1.0 / (width * n_tp)),
        [((3, le, hidden), F32), ((3, cols), F32)],
        pos, got_lines, other_lines, smem=1,
    )
    return token_grad, gate_grad.astype(BF).T, stack, jnp.swapaxes(shared, 1, 2), e_norm, s_norm


def solution(mesh):
    return jax.shard_map(
        body,
        mesh=mesh,
        in_specs=(
            P("ep", "tp"),
            P("ep", "tp"),
            P("ep", None),
            P("ep", None),
            P("ep", "tp", None),
            P("ep", "tp", None),
            P("ep", "tp", None),
            P("tp", None),
            P("tp", None),
            P("tp", None),
        ),
        out_specs=(
            P("ep", "tp"),
            P("ep", None),
            P(None, "ep", "tp", None),
            P(None, "tp", "ep"),
            P(None, "ep", None),
            P(None, "ep"),
        ),
        check_vma=False,
    )
```
